256 devices in a mesh: sp: 128 (over z, y, x), tp: 2 (over core).
Axes of the slice: x: 4, y: 4, z: 8, core: 2. Of those that a mesh axis runs over, the one named last changes fastest.
Arguments:
- conv_value: bfloat16 [65536, 1536], P('sp', 'tp'), may hold values from -6 to 6
- conv_gate: bfloat16 [65536, 1536], P('sp', 'tp'), may hold values from -8 to 8
- conv_out: bfloat16 [65536, 1536], P('sp', 'tp'), may hold values from -40 to 40
- conv_taps: bfloat16 [31, 1536], P(None, 'tp'), may hold values from -1 to 1
- norm_gain: float32 [1536], P('tp'), may hold values from 0.1 to 1.9
- norm_shift: float32 [1536], P('tp'), may hold values from -3 to 3
- proj_weight: bfloat16 [2048, 1536], P(None, 'tp'), may hold values from -0.15625 to 0.15625
- out_grad: bfloat16 [65536, 2048], P('sp'), may hold values from -24 to 24
Outputs:
- grad_value: bfloat16 [65536, 1536], P('sp', 'tp')
- grad_gate: bfloat16 [65536, 1536], P('sp', 'tp')
- grad_taps: float32 [31, 1536], P(None, 'tp')
- grad_gain: float32 [1536], P('tp')
- grad_shift: float32 [1536], P('tp')
- grad_proj: float32 [2048, 1536], P('sp', 'tp')
The draws below stay inside these ranges and needn't reach their ends.
All inputs are finite; a program needn't handle non-finite values.
Results may differ from the reference program's by a relative error of at most 0.005.
Values may be sent and summed in bfloat16 or wider, within the bound.
A program may use at most 64 MiB of HBM per device.

```python
import jax
import jax.numpy as jnp
from jax import lax

D = 2048
CH = 1536
TAPS = 31
SEQ = 65536


def draw_conv_out(key, part):
    key_scale, key_group, key_base, key_mean = jax.random.split(key, 4)
    chan_scale = jnp.exp(jax.random.uniform(key_scale, (CH,), jnp.float32, -1.0, 1.0))
    group_scale = jnp.exp(jax.random.uniform(key_group, (8,), jnp.float32, -1.2, 1.2))
    group_index = jnp.arange(CH) * 8 // CH
    scales = chan_scale * group_scale[group_index]
    base = jax.random.normal(key_base, (SEQ, CH), jnp.float32) * scales
    offset = jax.random.normal(key_mean, (SEQ, 1), jnp.float32)
    return jnp.clip(base + offset, -40.0, 40.0).astype(jnp.bfloat16)


def spiked(values, rng, source, target, parts, factor):
    def block_of(position):
        return (jnp.arange(values.shape[position]) // (values.shape[position] // parts)).reshape((-1,) + (1,) * (values.ndim - 1 - position))

    one_side = jax.random.permutation(rng, parts)[block_of(target)]
    other_side = (block_of(target) + parts // 2) % parts
    return jnp.where((block_of(source) == one_side) | (block_of(source) == other_side), factor * values, values)


def steps_of(stream_key, extent, shards, smallest, high):
    def one(axis_at, parts):
        steps = jax.random.uniform(jax.random.fold_in(jax.random.fold_in(stream_key, 6), axis_at), (parts,), jnp.float32, smallest / len(shards), high / len(shards))
        return jnp.repeat(jnp.exp(steps), extent[axis_at] // parts).reshape((-1,) + (1,) * (len(extent) - axis_at - 1))

    factor_of = one(*shards[0])
    for cut in shards[1:]:
        factor_of = factor_of * one(*cut)
    return factor_of


def bell_draw(own_key, dims, scale, limit, cuts=(), held_as=jnp.bfloat16):
    entries = jax.random.normal(own_key, dims, jnp.float32) * scale
    if len(cuts) > 0:
        entries = steps_of(own_key, dims, cuts, -0.22, 0.18) * entries
    return jnp.clip(entries, min=-limit, max=limit).astype(held_as)


def noise_with(key, extent, spread, reach, pieces, heavy, held_as=jnp.bfloat16):
    drawn = spread * jax.random.normal(key, extent, jnp.float32)
    if pieces:
        drawn = drawn * steps_of(key, extent, pieces, -0.22, 0.18)
    return jnp.clip(spiked(drawn, jax.random.fold_in(key, 3), *heavy), -reach, reach).astype(held_as)


def setup_inputs(seed: int = 0) -> dict:
    splits = jax.random.split(jax.random.key(seed), 9)
    return {
        "conv_value": bell_draw(splits[0], (SEQ, CH), 1.0, 6.0, ((0, 128), (1, 2))),
        "conv_gate": bell_draw(splits[1], (SEQ, CH), 1.5, 8.0, ((0, 128), (1, 2))),
        "conv_out": draw_conv_out(jax.random.fold_in(splits[8], 71), 0),
        "conv_taps": bell_draw(splits[3], (TAPS, CH), TAPS ** -0.5, 1.0, ((1, 2),)),
        "norm_gain": jnp.clip(1.0 + 0.18 * jax.random.normal(splits[4], (CH,), jnp.float32), 0.1, 1.9),
        "norm_shift": bell_draw(splits[5], (CH,), 0.5, 3.0, ((0, 2),), jnp.float32),
        "proj_weight": bell_draw(splits[6], (D, CH), CH ** -0.5, 0.15625, ((1, 2),)),
        "out_grad": noise_with(splits[7], (SEQ, D), 1.0, 24.0, ((0, 128),), (0, 1, 128, 5.5)),
    }


norm_eps = 1e-05

def reference(conv_value, conv_gate, conv_out, conv_taps, norm_gain, norm_shift, proj_weight, out_grad):
    height = conv_out.astype(jnp.float32)
    center = lax.optimization_barrier(jnp.mean(height, axis=1, keepdims=True))
    centered = height - center
    variance = lax.optimization_barrier(jnp.mean(centered * centered, axis=1, keepdims=True))
    inv_std = lax.rsqrt(variance + norm_eps)
    normed = centered * inv_std
    shifted = normed * norm_gain + norm_shift
    sig_norm = jax.nn.sigmoid(shifted)
    active = (shifted * sig_norm).astype(jnp.bfloat16)
    grad_proj = jnp.dot(out_grad.T, active, preferred_element_type=jnp.float32)
    act_grad = jnp.dot(out_grad, proj_weight, preferred_element_type=jnp.float32)
    norm_grad = act_grad * (sig_norm * (1.0 + shifted * (1.0 - sig_norm)))
    grad_gain = lax.optimization_barrier(jnp.sum(norm_grad * normed, axis=0))
    grad_shift = lax.optimization_barrier(jnp.sum(norm_grad, axis=0))
    scaled = norm_grad * norm_gain
    height_grad = inv_std * (scaled - lax.optimization_barrier(jnp.mean(scaled, axis=1, keepdims=True)) - normed * lax.optimization_barrier(jnp.mean(scaled * normed, axis=1, keepdims=True)))
    sig_gate = jax.nn.sigmoid(conv_gate.astype(jnp.float32))
    value_float = conv_value.astype(jnp.float32)
    gated_rows = lax.optimization_barrier((value_float * sig_gate).astype(jnp.bfloat16)).astype(jnp.float32)
    tap_reach = TAPS - 1
    padded_rows = jnp.pad(gated_rows, ((tap_reach, 0), (0, 0)))
    padded_grad = jnp.pad(height_grad, ((0, tap_reach), (0, 0)))
    tap_values = conv_taps.astype(jnp.float32)
    tap_list = []
    gated_grad = jnp.zeros_like(height_grad)
    for tap_index in range(TAPS):
        tap_list.append(lax.optimization_barrier(jnp.sum(height_grad * padded_rows[tap_index:tap_index + SEQ], axis=0)))
        begin = tap_reach - tap_index
        gated_grad = gated_grad + tap_values[tap_index] * padded_grad[begin:begin + SEQ]
    grad_taps = jnp.stack(tap_list)
    grad_value = (gated_grad * sig_gate).astype(jnp.bfloat16)
    grad_gate = (gated_grad * value_float * sig_gate * (1.0 - sig_gate)).astype(jnp.bfloat16)
    return (grad_value, grad_gate, grad_taps, grad_gain, grad_shift, grad_proj)
```

```python
import functools

import jax
import jax.numpy as jnp
from jax import lax
from jax.experimental import pallas as pl
from jax.experimental.pallas import tpu as pltpu
from jax.sharding import Mesh
from jax.sharding import PartitionSpec as P

MESH = pl.DeviceIdType.MESH
F32 = jnp.float32
BF16 = jnp.bfloat16
SP = ("z", "y", "x")
EPS = 1e-05
HALO = 32
LANE = 128
TILE = 32


class Slots:
    def __init__(self):
        self.used = 0

    def take(self, count):
        first = self.used
        self.used += count
        return first


def layout(nz, ny, nx):
    slots = Slots()
    plane = ny * nx
    return slots, {
        "stat": slots.take(1),
        "sums": slots.take(1),
        "gated": slots.take(1),
        "height": slots.take(1),
        "x1": slots.take(nx - 1),
        "y1": slots.take(ny - 1),
        "x2": slots.take(ny - 1),
        "y2": slots.take(nx - 1),
        "x3": slots.take(nz - 1),
        "y3": slots.take(nz - 1),
        "zr": slots.take(nz // 2),
        "zl": slots.take(nz // 2),
        "z2": slots.take(nx - 1),
        "z3": slots.take(ny - 1),
        "a1": slots.take(plane - 1),
        "a2": slots.take(nz),
        "a3": slots.take(plane - 1),
    }


def kernel(sizes, *refs):
    nz, ny, nx, rows, chan, depth, taps = sizes
    (cv_h, cg_h, co_h, taps_h, gain_h, shift_h, w_h, og_h, gv_o, gg_o, small_o, proj_o), rest = refs[:12], refs[12:]
    (co_v, og_v, w_v, cv_v, cg_v, taps_v, gain_v, shift_v, st_s, st_r, s2_s, s2_r, iv_v, sg_v, gt_v, nm_v, ds_v,
     act_v, ag_v, hg_v, gh_s, gh_r, hh_s, hh_r, px, py, pz, rx, ry, rzr, rzl, sx, sy, rx2, ry2, tx, ty, rx3, ry3,
     sz, rz2, tz, rz3, proj_v, sa, ra, fa, rza, fin, ag_a, small_v, gv_v, gg_v, in_sem, out_sem, ssem, rsem) = rest
    blocks = chan // LANE
    total = 2 * chan
    reach = taps - 1
    plane = ny * nx
    _, at = layout(nz, ny, nx)
    z, y, x, core = (lax.axis_index(a) for a in ("z", "y", "x", "tp"))
    place = y * nx + x
    line = z * plane + place
    count = nz * plane

    def where(index):
        return {"z": lax.div(index, plane), "y": lax.rem(lax.div(index, nx), ny), "x": lax.rem(index, nx)}

    after = where(lax.rem(line + 1, count))
    before = where(lax.rem(line + count - 1, count))
    other = {"tp": 1 - core}

    def along(axis, size, me, step):
        return {axis: lax.rem(me + step + size, size)}

    def in_plane(step):
        p = lax.rem(place + step, plane)
        return {"y": lax.div(p, nx), "x": lax.rem(p, nx)}

    def remote(src, dst, slot, target):
        return pltpu.make_async_remote_copy(
            src_ref=src, dst_ref=dst, send_sem=ssem.at[slot], recv_sem=rsem.at[slot],
            device_id=target, device_id_type=MESH)

    barrier = pltpu.get_barrier_semaphore()
    peers = [other, after, before]
    peers += [in_plane(o) for o in range(1, plane)]
    peers += [along("z", nz, z, o) for o in range(1, nz)]
    for peer in peers:
        pl.semaphore_signal(barrier, inc=1, device_id=peer, device_id_type=MESH)

    loads = {}
    for slot, (name, src, dst) in enumerate((
            ("co", co_h, co_v), ("gain", gain_h, gain_v), ("shift", shift_h, shift_v), ("cg", cg_h, cg_v),
            ("cv", cv_h, cv_v), ("og", og_h, og_v), ("w", w_h, w_v), ("taps", taps_h, taps_v))):
        loads[name] = pltpu.make_async_copy(src, dst, in_sem.at[slot])
        loads[name].start()

    lane = lax.broadcasted_iota(jnp.int32, (1, LANE), 1)
    first = lane < LANE // 2

    def lanes(b):
        return slice(b * LANE, (b + 1) * LANE)

    loads["co"].wait()

    def stats(i, carry):
        r = pl.ds(pl.multiple_of(i * 64, 64), 64)
        v = co_v[r, :].astype(F32)
        m = jnp.sum(v, axis=1, keepdims=True) * (1.0 / chan)
        d = v - m
        q = jnp.sum(d * d, axis=1, keepdims=True)
        st_s[r, :] = jnp.where(first, m, q)
        return carry

    lax.fori_loop(0, rows // 64, stats, 0)

    loads["cg"].wait()
    loads["cv"].wait()

    def gates(i, carry):
        r = pl.ds(pl.multiple_of(i * TILE, TILE), TILE)
        up = pl.ds(pl.multiple_of(i * TILE + HALO, TILE), TILE)
        for b in range(blocks):
            s = 0.5 * jnp.tanh(0.5 * cg_v[r, lanes(b)].astype(F32)) + 0.5
            sg_v[r, lanes(b)] = s
            gt_v[b, up, :] = (cv_v[r, lanes(b)].astype(F32) * s).astype(BF16).astype(F32)
        return carry

    lax.fori_loop(0, rows // TILE, gates, 0)
    for b in range(blocks):
        gh_s[:, lanes(b)] = gt_v[b, rows:rows + HALO, :].astype(BF16)

    pl.semaphore_wait(barrier, len(peers))
    stat_copy = remote(st_s, st_r, at["stat"], other)
    stat_copy.start()
    gated_copy = remote(gh_s, gh_r, at["gated"], after)
    gated_copy.start()

    loads["og"].wait()
    loads["w"].wait()

    def back(i, carry):
        r = pl.ds(pl.multiple_of(i * 128, 128), 128)
        ag_v[r, :] = jnp.dot(og_v[r, :], w_v[...], preferred_element_type=F32)
        return carry

    lax.fori_loop(0, rows // 128, back, 0)
    loads["gain"].wait()
    loads["shift"].wait()
    stat_copy.wait_recv()

    def norm(i, carry):
        r = pl.ds(pl.multiple_of(i * TILE, TILE), TILE)
        mine, theirs = st_s[r, :], st_r[r, :]
        m1, q1 = mine[:, 0:1], mine[:, 64:65]
        m2, q2 = theirs[:, 0:1], theirs[:, 64:65]
        gap = m1 - m2
        mean = 0.5 * (m1 + m2)
        inv = lax.rsqrt((q1 + q2 + gap * gap * (chan / 2)) * (1.0 / total) + EPS)
        inv = jnp.broadcast_to(inv, (TILE, LANE))
        mean = jnp.broadcast_to(mean, (TILE, LANE))
        iv_v[r, :] = inv
        for b in range(blocks):
            n = (co_v[r, lanes(b)].astype(F32) - mean) * inv
            s = n * gain_v[:, lanes(b)] + shift_v[:, lanes(b)]
            sig = 0.5 * jnp.tanh(0.5 * s) + 0.5
            a = s * sig
            act_v[r, lanes(b)] = a.astype(BF16)
            nm_v[r, lanes(b)] = n
            ds_v[r, lanes(b)] = sig + a * (1.0 - sig)
        return carry

    lax.fori_loop(0, rows // TILE, norm, 0)

    third = chan // 3
    span = plane * 16
    half = ny // 2

    def z_first(step_slot, src_z, part, direction):
        buf, base = (rzr, at["zr"]) if direction > 0 else (rzl, at["zl"])
        src, dst = pz.at[src_z], buf.at[step_slot]
        if part is not None:
            src, dst = src.at[part], dst.at[part]
        return remote(src, dst, base + step_slot, along("z", nz, z, direction))

    upper, lower = pl.ds(0, half), pl.ds(half, half)

    def project(k, carry):
        away = nz // 2 - lax.div(k + 1, 2)
        sign = 2 * lax.rem(k, 2) - 1
        zz = lax.rem(z + sign * away + nz, nz)
        cols = pl.ds(pl.multiple_of(zz * span, span), span)
        block = lax.dot_general(og_v[:, cols], act_v[...], (((0,), (0,)), ((), ())), preferred_element_type=F32)
        block = block.astype(BF16)
        for yy in range(ny):
            for xx in range(nx):
                part = slice((yy * nx + xx) * 16, (yy * nx + xx) * 16 + 16)
                px[xx, zz, yy] = block[part, 0:third]
                py[yy, zz, xx] = block[part, third:2 * third]
                pz[zz, yy, xx] = block[part, 2 * third:]
        for o in range(1, nx):
            peer = along("x", nx, x, o)
            remote(px.at[peer["x"], zz], rx.at[o - 1, zz], at["x1"] + o - 1, peer).start()
        for o in range(1, ny):
            peer = along("y", ny, y, o)
            remote(py.at[peer["y"], zz], ry.at[o - 1, zz], at["y1"] + o - 1, peer).start()

        @pl.when(k == 0)
        def _():
            z_first(0, zz, upper, 1).start()
            z_first(0, zz, lower, -1).start()

        return carry

    lax.fori_loop(0, nz, project, 0)

    def grads(i, carry):
        r = pl.ds(pl.multiple_of(i * TILE, TILE), TILE)
        carry = list(carry)
        row_sum = jnp.zeros((TILE, LANE), F32)
        row_dot = jnp.zeros((TILE, LANE), F32)
        for b in range(blocks):
            g = ag_v[r, lanes(b)] * ds_v[r, lanes(b)]
            n = nm_v[r, lanes(b)]
            gn = g * n
            carry[b] = carry[b] + jnp.sum(gn.reshape(TILE // 8, 8, LANE), axis=0)
            carry[blocks + b] = carry[blocks + b] + jnp.sum(g.reshape(TILE // 8, 8, LANE), axis=0)
            gain = gain_v[:, lanes(b)]
            s = g * gain
            ag_v[r, lanes(b)] = s
            row_sum = row_sum + s
            row_dot = row_dot + gn * gain
        sums = jnp.sum(row_sum, axis=1, keepdims=True)
        dots = jnp.sum(row_dot, axis=1, keepdims=True)
        s2_s[r, :] = jnp.where(first, sums, dots)
        return tuple(carry)

    partial = lax.fori_loop(0, rows // TILE, grads, tuple(jnp.zeros((8, LANE), F32) for _ in range(2 * blocks)))
    sums_copy = remote(s2_s, s2_r, at["sums"], other)
    sums_copy.start()

    z_recv = []

    def z_step(step):
        for direction in (1, -1):
            dest = lax.rem(z + direction * (nz // 2 - step) + nz, nz)
            part = None
            if step == 1:
                part = upper if direction > 0 else lower
            z_first(step - 1, dest, part, direction).wait_recv()
            buf = rzr if direction > 0 else rzl
            ys = range(ny) if step > 1 else (range(half) if direction > 0 else range(half, ny))
            for yy in ys:
                pz[dest, yy] = (pz[dest, yy].astype(F32) + buf[step - 1, yy].astype(F32)).astype(BF16)
            z_first(step, dest, None, direction).start()

    z_step(1)

    gated_copy.wait_recv()
    for b in range(blocks):
        head = gh_r[:, lanes(b)].astype(F32)
        gt_v[b, 0:HALO, :] = jnp.where(line == 0, 0.0, head)

    sums_copy.wait_recv()

    def height(i, carry):
        r = pl.ds(pl.multiple_of(i * TILE, TILE), TILE)
        both = (s2_s[r, :] + s2_r[r, :]) * (1.0 / total)
        sums = jnp.broadcast_to(both[:, 0:1], (TILE, LANE))
        dots = jnp.broadcast_to(both[:, 64:65], (TILE, LANE))
        inv = iv_v[r, :]
        for b in range(blocks):
            hg_v[b, r, :] = inv * (ag_v[r, lanes(b)] - sums - nm_v[r, lanes(b)] * dots)
        return carry

    lax.fori_loop(0, rows // TILE, height, 0)
    for b in range(blocks):
        hh_s[:, lanes(b)] = hg_v[b, 0:HALO, :].astype(BF16)
    height_copy = remote(hh_s, hh_r, at["height"], before)
    height_copy.start()

    small_rows = (taps + 2 + 7) // 8
    flat = sa.shape[0] * sa.shape[1]

    def tap_block(b):
        def step(t, acc):
            base = t * 8
            h = hg_v[b, pl.ds(pl.multiple_of(base, 8), 8), :]
            return tuple(
                acc[j] + h * gt_v[b, pl.ds(base + (HALO - reach) + j, 8), :] for j in range(taps))

        acc = lax.fori_loop(0, rows // 8, step, tuple(jnp.zeros((8, LANE), F32) for _ in range(taps)))
        acc = list(acc) + [partial[b], partial[blocks + b]]
        lines = [jnp.sum(a, axis=0, keepdims=True) for a in acc]
        lines += [jnp.zeros((1, LANE), F32)] * (small_rows * 8 - len(lines))
        for t in range(small_rows):
            tile = b * small_rows + t
            sa[tile // 2, tile % 2] = jnp.concatenate(lines[t * 8:t * 8 + 8], axis=0)

    for b in range(blocks):
        tap_block(b)
        if b == 1:
            z_step(2)
        if b == 4:
            z_step(3)
    for tile in range(blocks * small_rows, flat):
        sa[tile // 2, tile % 2] = jnp.zeros((8, LANE), F32)
    for o in range(1, plane):
        remote(sa.at[lax.rem(place + o, plane)], ra.at[o - 1], at["a1"] + o - 1, in_plane(o)).start()

    def gather_x(wide, me, got, out, name, axis, size, own_axis_size):
        for o in range(1, own_axis_size):
            remote(wide.at[me], got.at[o - 1], at[name + "1"] + o - 1, other).wait_recv()

        def step(zz, carry):
            v = wide[me, zz].astype(F32)
            for o in range(own_axis_size - 1):
                v = v + got[o, zz].astype(F32)
            v = v.astype(BF16)
            for w in range(size):
                out[w, zz] = v[w]
            return carry

        lax.fori_loop(0, nz, step, 0)

    gather_x(px, x, rx, sx, "x", "y", ny, nx)
    for o in range(1, ny):
        peer = along("y", ny, y, o)
        remote(sx.at[peer["y"]], rx2.at[o - 1], at["x2"] + o - 1, peer).start()
    gather_x(py, y, ry, sy, "y", "x", nx, ny)
    for o in range(1, nx):
        peer = along("x", nx, x, o)
        remote(sy.at[peer["x"]], ry2.at[o - 1], at["y2"] + o - 1, peer).start()

    def z_done():
        z_first(nz // 2 - 1, z, None, 1).wait_recv()
        z_first(nz // 2 - 1, z, None, -1).wait_recv()
        for yy in range(ny):
            v = pz[z, yy].astype(F32) + rzr[nz // 2 - 1, yy].astype(F32) + rzl[nz // 2 - 1, yy].astype(F32)
            v = v.astype(BF16)
            for xx in range(nx):
                sz[xx, yy] = v[xx]
        for o in range(1, nx):
            peer = along("x", nx, x, o)
            remote(sz.at[peer["x"]], rz2.at[o - 1], at["z2"] + o - 1, peer).start()

    def small_plane():
        for o in range(1, plane):
            remote(sa.at[0], ra.at[o - 1], at["a1"] + o - 1, in_plane(o)).wait_recv()
        v = sa[place]
        for o in range(plane - 1):
            v = v + ra[o]
        fa[...] = v
        rza[z] = v
        for o in range(1, nz):
            remote(fa, rza.at[z], at["a2"] + z, along("z", nz, z, o)).start()

    def xy_third(own, me, got, out, last, name, size):
        for o in range(1, size):
            remote(own.at[0], got.at[o - 1], at[name + "2"] + o - 1, other).wait_recv()
        v = own[me].astype(F32)
        for o in range(size - 1):
            v = v + got[o].astype(F32)
        out[...] = v.astype(BF16)
        for o in range(1, nz):
            peer = along("z", nz, z, o)
            remote(out.at[peer["z"]], last.at[o - 1], at[name + "3"] + o - 1, peer).start()

    def z_third():
        for o in range(1, nx):
            remote(sz.at[0], rz2.at[o - 1], at["z2"] + o - 1, other).wait_recv()
        v = sz[x].astype(F32)
        for o in range(nx - 1):
            v = v + rz2[o].astype(F32)
        tz[...] = v.astype(BF16)
        for o in range(1, ny):
            peer = along("y", ny, y, o)
            remote(tz.at[peer["y"]], rz3.at[o - 1], at["z3"] + o - 1, peer).start()

    def small_line():
        for o in range(1, nz):
            zz = lax.rem(z + o, nz)
            remote(fa, rza.at[zz], at["a2"] + zz, other).wait_recv()
        v = rza[0]
        for zz in range(1, nz):
            v = v + rza[zz]
        fin[...] = v
        ag_a[place] = v
        for o in range(1, plane):
            remote(fin, ag_a.at[place], at["a3"] + o - 1, in_plane(o)).start()

    height_copy.wait_recv()
    for b in range(blocks):
        tail = hh_r[:, lanes(b)].astype(F32)
        hg_v[b, rows:rows + HALO, :] = jnp.where(line == count - 1, 0.0, tail)

    loads["taps"].wait()

    def gated_block(b):
        lines = taps_v[:, lanes(b)].astype(F32)
        spread = [jnp.broadcast_to(lines[j:j + 1, :], (8, LANE)) for j in range(taps)]

        def step(t, carry):
            base = t * 16
            r = pl.ds(pl.multiple_of(base, 16), 16)
            pieces = []
            for u in range(2):
                acc = None
                for j in range(taps):
                    term = spread[j] * hg_v[b, pl.ds(base + 8 * u + reach - j, 8), :]
                    acc = term if acc is None else acc + term
                pieces.append(acc)
            g = jnp.concatenate(pieces, axis=0)
            s = sg_v[r, lanes(b)]
            gs = g * s
            gv_v[r, lanes(b)] = gs.astype(BF16)
            gg_v[r, lanes(b)] = (gs * cv_v[r, lanes(b)].astype(F32) * (1.0 - s)).astype(BF16)
            return carry

        lax.fori_loop(0, rows // 16, step, 0)

    outs = []
    for b in range(blocks):
        gated_block(b)
        if b == 0:
            z_done()
        if b == 1:
            xy_third(sx, y, rx2, tx, rx3, "x", ny)
            xy_third(sy, x, ry2, ty, ry3, "y", nx)
        if b == 2:
            small_plane()
        if b == 3:
            z_third()
        if b == 5:
            small_line()

    outs.append(pltpu.make_async_copy(gv_v, gv_o, out_sem.at[0]))
    outs.append(pltpu.make_async_copy(gg_v, gg_o, out_sem.at[1]))
    for c in outs:
        c.start()

    for buf, own, last, name in ((0, tx, rx3, "x3"), (1, ty, ry3, "y3")):
        for o in range(1, nz):
            remote(own.at[0], last.at[o - 1], at[name] + o - 1, other).wait_recv()
        v = own[z].astype(F32)
        for o in range(nz - 1):
            v = v + last[o].astype(F32)
        proj_v[:, buf * third:(buf + 1) * third] = v
    for o in range(1, ny):
        remote(tz.at[0], rz3.at[o - 1], at["z3"] + o - 1, other).wait_recv()
    v = tz[y].astype(F32)
    for o in range(ny - 1):
        v = v + rz3[o].astype(F32)
    proj_v[:, 2 * third:] = v
    outs.append(pltpu.make_async_copy(proj_v, proj_o, out_sem.at[2]))
    outs[-1].start()

    for o in range(1, plane):
        p = lax.rem(place - o + plane, plane)
        remote(fin, ag_a.at[p], at["a3"] + o - 1, other).wait_recv()
    for b in range(blocks):
        for t in range(small_rows):
            tile = b * small_rows + t
            small_v[t * 8:t * 8 + 8, lanes(b)] = ag_a[tile // 2, tile % 2]
    outs.append(pltpu.make_async_copy(small_v, small_o, out_sem.at[3]))
    outs[-1].start()

    stat_copy.wait_send()
    gated_copy.wait_send()
    sums_copy.wait_send()
    height_copy.wait_send()
    for o in range(nx - 1):
        remote(px.at[0], rx.at[o], at["x1"] + o, other).wait_send()
        remote(sy.at[0], ry2.at[o], at["y2"] + o, other).wait_send()
        remote(sz.at[0], rz2.at[o], at["z2"] + o, other).wait_send()
    for o in range(ny - 1):
        remote(py.at[0], ry.at[o], at["y1"] + o, other).wait_send()
        remote(sx.at[0], rx2.at[o], at["x2"] + o, other).wait_send()
        remote(tz.at[0], rz3.at[o], at["z3"] + o, other).wait_send()
    for o in range(nz - 1):
        remote(tx.at[0], rx3.at[o], at["x3"] + o, other).wait_send()
        remote(ty.at[0], ry3.at[o], at["y3"] + o, other).wait_send()
    for step in range(nz // 2):
        z_first(step, z, upper if step == 0 else None, 1).wait_send()
        z_first(step, z, lower if step == 0 else None, -1).wait_send()
    for o in range(plane - 1):
        remote(sa.at[0], ra.at[o], at["a1"] + o, other).wait_send()
        remote(fin, ag_a.at[0], at["a3"] + o, other).wait_send()
    for o in range(1, nz):
        remote(fa, rza.at[z], at["a2"] + z, other).wait_send()
    for c in outs:
        c.wait()


def local(conv_value, conv_gate, conv_out, conv_taps, norm_gain, norm_shift, proj_weight, out_grad):
    nz, ny, nx = (lax.axis_size(a) for a in SP)
    rows, chan = conv_value.shape
    depth = out_grad.shape[1]
    taps = conv_taps.shape[0]
    blocks = chan // LANE
    third = chan // 3
    plane = ny * nx
    slots, _ = layout(nz, ny, nx)
    vm = pltpu.VMEM
    small_rows = (taps + 2 + 7) // 8 * 8
    per = -(-blocks * small_rows // 8 // plane)
    scratch = [
        vm((rows, chan), BF16), vm((rows, depth), BF16), vm((depth, chan), BF16), vm((rows, chan), BF16),
        vm((rows, chan), BF16), vm((taps, chan), BF16), vm((1, chan), F32), vm((1, chan), F32),
        vm((rows, LANE), F32), vm((rows, LANE), F32), vm((rows, LANE), F32), vm((rows, LANE), F32),
        vm((rows, LANE), F32), vm((rows, chan), F32), vm((blocks, rows + HALO, LANE), F32), vm((rows, chan), F32),
        vm((rows, chan), F32), vm((rows, chan), BF16), vm((rows, chan), F32), vm((blocks, rows + HALO, LANE), F32),
        vm((HALO, chan), BF16), vm((HALO, chan), BF16), vm((HALO, chan), BF16), vm((HALO, chan), BF16),
        vm((nx, nz, ny, 16, third), BF16), vm((ny, nz, nx, 16, third), BF16), vm((nz, ny, nx, 16, third), BF16),
        vm((nx - 1, nz, ny, 16, third), BF16), vm((ny - 1, nz, nx, 16, third), BF16),
        vm((nz // 2, ny, nx, 16, third), BF16), vm((nz // 2, ny, nx, 16, third), BF16),
        vm((ny, nz, 16, third), BF16), vm((nx, nz, 16, third), BF16),
        vm((ny - 1, nz, 16, third), BF16), vm((nx - 1, nz, 16, third), BF16),
        vm((nz, 16, third), BF16), vm((nz, 16, third), BF16),
        vm((nz - 1, 16, third), BF16), vm((nz - 1, 16, third), BF16),
        vm((nx, ny, 16, third), BF16), vm((nx - 1, ny, 16, third), BF16),
        vm((ny, 16, third), BF16), vm((ny - 1, 16, third), BF16),
        vm((16, chan), F32),
        vm((plane, per, 8, LANE), F32), vm((plane - 1, per, 8, LANE), F32), vm((per, 8, LANE), F32),
        vm((nz, per, 8, LANE), F32), vm((per, 8, LANE), F32), vm((plane, per, 8, LANE), F32),
        vm((small_rows, chan), F32), vm((rows, chan), BF16), vm((rows, chan), BF16),
        pltpu.SemaphoreType.DMA((8,)), pltpu.SemaphoreType.DMA((4,)),
        pltpu.SemaphoreType.DMA((slots.used,)), pltpu.SemaphoreType.DMA((slots.used,)),
    ]
    anywhere = pl.BlockSpec(memory_space=pl.ANY)
    grad_value, grad_gate, small, grad_proj = pl.pallas_call(
        functools.partial(kernel, (nz, ny, nx, rows, chan, depth, taps)),
        out_shape=(
            jax.ShapeDtypeStruct((rows, chan), BF16),
            jax.ShapeDtypeStruct((rows, chan), BF16),
            jax.ShapeDtypeStruct((small_rows, chan), F32),
            jax.ShapeDtypeStruct((16, chan), F32),
        ),
        in_specs=[anywhere] * 8,
        out_specs=(anywhere,) * 4,
        scratch_shapes=scratch,
        compiler_params=pltpu.CompilerParams(
            collective_id=0, has_side_effects=True, vmem_limit_bytes=62 * 1024 * 1024),
        name="module_backward",
    )(conv_value, conv_gate, conv_out, conv_taps, norm_gain.reshape(1, chan), norm_shift.reshape(1, chan),
      proj_weight, out_grad)
    return grad_value, grad_gate, small[:taps], small[taps], small[taps + 1], grad_proj


def solution(mesh):
    split = Mesh(mesh.devices.reshape(8, 4, 4, mesh.shape["tp"]), (*SP, "tp"))
    placed = (
        P(SP, "tp"), P(SP, "tp"), P(SP, "tp"), P(None, "tp"), P("tp"), P("tp"), P(None, "tp"), P(SP, None),
    )
    return jax.shard_map(
        local,
        mesh=split,
        in_specs=placed,
        out_specs=(P(SP, "tp"), P(SP, "tp"), P(None, "tp"), P("tp"), P("tp"), P(SP, "tp")),
        check_vma=False,
    )
```

```python
import functools

import jax
import jax.numpy as jnp
from jax import lax
from jax.experimental import pallas as pl
from jax.experimental.pallas import tpu as pltpu
from jax.sharding import Mesh
from jax.sharding import PartitionSpec as P

MESH = pl.DeviceIdType.MESH
F32 = jnp.float32
BF16 = jnp.bfloat16
SP = ("z", "y", "x")
EPS = 1e-05
HALO = 32
LANE = 128
TILE = 32
GROUP = 4


class Slots:
    def __init__(self):
        self.used = 0

    def take(self, count):
        first = self.used
        self.used += count
        return first


def layout(nz, ny, nx):
    slots = Slots()
    plane = ny * nx
    return slots, {
        "stat": slots.take(1),
        "sums": slots.take(1),
        "gated": slots.take(1),
        "height": slots.take(1),
        "x1": slots.take(2 * (nx - 1)),
        "y1": slots.take(2 * (ny - 1)),
        "x2": slots.take(2 * (ny - 1)),
        "y2": slots.take(2 * (nx - 1)),
        "x3": slots.take(nz - 1),
        "y3": slots.take(nz - 1),
        "zr": slots.take(nz),
        "zl": slots.take(nz),
        "z2": slots.take(nx - 1),
        "z3": slots.take(ny - 1),
        "a1": slots.take(plane - 1),
        "a2": slots.take(nz),
        "a3": slots.take(plane - 1),
    }


def kernel(sizes, *refs):
    nz, ny, nx, rows, chan, depth, taps = sizes
    cv_h, cg_h, co_h, taps_h, gain_h, shift_h, w_h, og_h, gv_v, gg_v, taps_o, gain_o, shift_o, proj_v = refs[:14]
    (co_v, og_v, w_v, cv_v, cg_v, taps_v, gain_v, shift_v, st_s, st_r, s2_s, s2_r, iv_v, sg_v, gt_v, nm_v, ds_v,
     act_v, ag_v, hg_v, gh_s, gh_r, hh_s, hh_r, px, py, pz, rx, ry, rzr, rzl, sx, sy, rx2, ry2, tx, ty, rx3, ry3,
     sz, rz2, tz, rz3, sa, ra, fa, rza, fin, ag_a, in_sem, ssem, rsem) = refs[14:]
    blocks = chan // LANE
    total = 2 * chan
    reach = taps - 1
    plane = ny * nx
    _, at = layout(nz, ny, nx)
    z, y, x, core = (lax.axis_index(a) for a in ("z", "y", "x", "tp"))
    place = y * nx + x
    line = z * plane + place
    count = nz * plane

    def where(index):
        return {"z": lax.div(index, plane), "y": lax.rem(lax.div(index, nx), ny), "x": lax.rem(index, nx)}

    after = where(lax.rem(line + 1, count))
    before = where(lax.rem(line + count - 1, count))
    other = {"tp": 1 - core}

    def along(axis, size, me, step):
        return {axis: lax.rem(me + step + size, size)}

    def in_plane(step):
        p = lax.rem(place + step, plane)
        return {"y": lax.div(p, nx), "x": lax.rem(p, nx)}

    def remote(src, dst, slot, target):
        return pltpu.make_async_remote_copy(
            src_ref=src, dst_ref=dst, send_sem=ssem.at[slot], recv_sem=rsem.at[slot],
            device_id=target, device_id_type=MESH)

    loads = {}
    for slot, (name, src, dst) in enumerate((
            ("co", co_h, co_v), ("gain", gain_h, gain_v), ("shift", shift_h, shift_v), ("cg", cg_h, cg_v),
            ("cv", cv_h, cv_v), ("og", og_h, og_v), ("w", w_h, w_v), ("taps", taps_h, taps_v))):
        loads[name] = pltpu.make_async_copy(src, dst, in_sem.at[slot])
        loads[name].start()

    barrier = pltpu.get_barrier_semaphore()
    peers = [other, after, before]
    peers += [in_plane(o) for o in range(1, plane)]
    peers += [along("z", nz, z, o) for o in range(1, nz)]
    for peer in peers:
        pl.semaphore_signal(barrier, inc=1, device_id=peer, device_id_type=MESH)

    def lanes(b):
        return slice(b * LANE, (b + 1) * LANE)

    loads["co"].wait()

    wide = rows // 2

    def means(i, carry):
        for u in range(wide // 64):
            r = pl.ds(pl.multiple_of(i * wide + u * 64, 64), 64)
            m = jnp.sum(co_v[r, :].astype(F32), axis=1, keepdims=True) * (1.0 / chan)
            st_s[0, r, :] = jnp.broadcast_to(m, (64, LANE))
        return carry

    lax.fori_loop(0, 2, means, 0)

    def spreads(i, carry):
        for u in range(wide // 64):
            r = pl.ds(pl.multiple_of(i * wide + u * 64, 64), 64)
            m = st_s[0, r, :]
            q = jnp.zeros((64, LANE), F32)
            for b in range(blocks):
                d = co_v[r, lanes(b)].astype(F32) - m
                q = q + d * d
            st_s[1, r, :] = jnp.broadcast_to(jnp.sum(q, axis=1, keepdims=True), (64, LANE))
        return carry

    lax.fori_loop(0, 2, spreads, 0)

    loads["cg"].wait()
    loads["cv"].wait()

    def gates(i, carry):
        r = pl.ds(pl.multiple_of(i * TILE, TILE), TILE)
        up = pl.ds(pl.multiple_of(i * TILE + HALO, TILE), TILE)
        for b in range(blocks):
            s = 0.5 * jnp.tanh(0.5 * cg_v[r, lanes(b)].astype(F32)) + 0.5
            sg_v[r, lanes(b)] = s
            gt_v[b, up, :] = (cv_v[r, lanes(b)].astype(F32) * s).astype(BF16).astype(F32)
        return carry

    lax.fori_loop(0, rows // TILE, gates, 0)
    for b in range(blocks):
        gh_s[:, lanes(b)] = gt_v[b, rows:rows + HALO, :].astype(BF16)

    pl.semaphore_wait(barrier, len(peers))
    stat_copy = remote(st_s, st_r, at["stat"], other)
    stat_copy.start()
    gated_copy = remote(gh_s, gh_r, at["gated"], after)
    gated_copy.start()

    loads["gain"].wait()
    loads["shift"].wait()
    stat_copy.wait_recv()

    def norm(i, carry):
        r = pl.ds(pl.multiple_of(i * TILE, TILE), TILE)
        m1, m2 = st_s[0, r, :], st_r[0, r, :]
        gap = m1 - m2
        mean = 0.5 * (m1 + m2)
        inv = lax.rsqrt((st_s[1, r, :] + st_r[1, r, :] + gap * gap * (chan / 2)) * (1.0 / total) + EPS)
        iv_v[r, :] = inv
        for b in range(blocks):
            n = (co_v[r, lanes(b)].astype(F32) - mean) * inv
            s = n * gain_v[lanes(b)].reshape(1, LANE) + shift_v[lanes(b)].reshape(1, LANE)
            sig = 0.5 * jnp.tanh(0.5 * s) + 0.5
            a = s * sig
            act_v[r, lanes(b)] = a.astype(BF16)
            nm_v[r, lanes(b)] = n
            ds_v[r, lanes(b)] = sig + a * (1.0 - sig)
        return carry

    lax.fori_loop(0, rows // TILE, norm, 0)

    third = chan // 3
    span = plane * 16
    half = ny // 2
    stretches = ((0, nz // 2 + 1), (nz // 2 + 1, nz))
    upper, lower = pl.ds(0, half), pl.ds(half, half)

    def far(k):
        away = nz // 2 - lax.div(k + 1, 2)
        return lax.rem(z + (2 * lax.rem(k, 2) - 1) * away + nz, nz)

    def ring(step, leads, src_z, direction):
        buf, base = (rzr, at["zr"]) if direction > 0 else (rzl, at["zl"])
        part = upper if leads == (direction > 0) else lower
        slot = base + 2 * step + (0 if leads else 1)
        return remote(pz.at[src_z, part], buf.at[step, part], slot, along("z", nz, z, direction))

    def project(stretch):
        def step(k, carry):
            zz = far(k)
            cols = pl.ds(pl.multiple_of(zz * span, span), span)
            block = lax.dot_general(og_v[:, cols], act_v[...], (((0,), (0,)), ((), ())), preferred_element_type=F32)
            block = block.astype(BF16)
            for yy in range(ny):
                for xx in range(nx):
                    part = slice((yy * nx + xx) * 16, (yy * nx + xx) * 16 + 16)
                    px[xx, zz, yy] = block[part, 0:third]
                    py[yy, zz, xx] = block[part, third:2 * third]
                    pz[zz, yy, xx] = block[part, 2 * third:]
            for o in range(1, nx):
                peer = along("x", nx, x, o)
                slot = at["x1"] + stretch * (nx - 1) + o - 1
                remote(px.at[peer["x"], zz], rx.at[o - 1, zz], slot, peer).start()
            for o in range(1, ny):
                peer = along("y", ny, y, o)
                slot = at["y1"] + stretch * (ny - 1) + o - 1
                remote(py.at[peer["y"], zz], ry.at[o - 1, zz], slot, peer).start()
            if stretch == 0:
                @pl.when(k == 0)
                def _():
                    ring(0, True, zz, 1).start()
                    ring(0, True, zz, -1).start()

                @pl.when(k == 1)
                def _():
                    ring(1, False, zz, 1).start()

                @pl.when(k == 2)
                def _():
                    ring(1, False, zz, -1).start()

            return carry

        lax.fori_loop(*stretches[stretch], step, 0)

    def z_step(step, leads):
        for direction in (1, -1):
            dest = lax.rem(z + direction * (nz // 2 - step) + nz, nz)
            ring(step - 1, leads, dest, direction).wait_recv()
            buf = rzr if direction > 0 else rzl
            for yy in (range(half) if leads == (direction > 0) else range(half, ny)):
                pz[dest, yy] = (pz[dest, yy].astype(F32) + buf[step - 1, yy].astype(F32)).astype(BF16)
            ring(step, leads, dest, direction).start()

    loads["og"].wait()
    project(0)

    loads["w"].wait()

    def back(i, carry):
        r = pl.ds(pl.multiple_of(i * 128, 128), 128)
        ag_v[r, :] = jnp.dot(og_v[r, :], w_v[...], preferred_element_type=F32)
        return carry

    lax.fori_loop(0, rows // 128, back, 0)
    z_step(1, True)

    def grads(i, carry):
        r = pl.ds(pl.multiple_of(i * TILE, TILE), TILE)
        carry = list(carry)
        row_sum = jnp.zeros((TILE, LANE), F32)
        row_dot = jnp.zeros((TILE, LANE), F32)
        for b in range(blocks):
            g = ag_v[r, lanes(b)] * ds_v[r, lanes(b)]
            n = nm_v[r, lanes(b)]
            gn = g * n
            carry[b] = carry[b] + jnp.sum(gn.reshape(TILE // 8, 8, LANE), axis=0)
            carry[blocks + b] = carry[blocks + b] + jnp.sum(g.reshape(TILE // 8, 8, LANE), axis=0)
            gain = gain_v[lanes(b)].reshape(1, LANE)
            s = g * gain
            ag_v[r, lanes(b)] = s
            row_sum = row_sum + s
            row_dot = row_dot + gn * gain
        s2_s[0, r, :] = row_sum
        s2_s[1, r, :] = row_dot
        return tuple(carry)

    partial = lax.fori_loop(0, rows // TILE, grads, tuple(jnp.zeros((8, LANE), F32) for _ in range(2 * blocks)))

    def channel_sums(i, carry):
        for u in range(wide // 64):
            r = pl.ds(pl.multiple_of(i * wide + u * 64, 64), 64)
            for w in range(2):
                v = jnp.sum(s2_s[w, r, :], axis=1, keepdims=True)
                s2_s[w, r, :] = jnp.broadcast_to(v, (64, LANE))
        return carry

    lax.fori_loop(0, 2, channel_sums, 0)
    sums_copy = remote(s2_s, s2_r, at["sums"], other)
    sums_copy.start()

    project(1)
    z_step(2, False)

    gated_copy.wait_recv()
    for b in range(blocks):
        head = gh_r[:, lanes(b)].astype(F32)
        gt_v[b, 0:HALO, :] = jnp.where(line == 0, 0.0, head)

    sums_copy.wait_recv()

    def height(i, carry):
        r = pl.ds(pl.multiple_of(i * TILE, TILE), TILE)
        sums = (s2_s[0, r, :] + s2_r[0, r, :]) * (1.0 / total)
        dots = (s2_s[1, r, :] + s2_r[1, r, :]) * (1.0 / total)
        inv = iv_v[r, :]
        for b in range(blocks):
            hg_v[b, r, :] = inv * (ag_v[r, lanes(b)] - sums - nm_v[r, lanes(b)] * dots)
        return carry

    lax.fori_loop(0, rows // TILE, height, 0)
    for b in range(blocks):
        hh_s[:, lanes(b)] = hg_v[b, 0:HALO, :].astype(BF16)
    height_copy = remote(hh_s, hh_r, at["height"], before)
    height_copy.start()

    z_step(2, True)

    def gather(stretch, wide, me, got, out, got2, name, axis, size, own_size, own_me):
        lo, hi = stretches[stretch]
        for o in range(1, own_size):
            slot = at[name + "1"] + stretch * (own_size - 1) + o - 1
            part = got.at[o - 1, pl.ds(0, hi - lo)]
            remote(part, part, slot, other).wait_recv()

        def step(k, carry):
            zz = far(k)
            v = wide[me, zz].astype(F32)
            for o in range(own_size - 1):
                v = v + got[o, zz].astype(F32)
            v = v.astype(BF16)
            for w in range(size):
                out[w, zz] = v[w]
            for o in range(1, size):
                peer = along(axis, size, own_me, o)
                slot = at[name + "2"] + stretch * (size - 1) + o - 1
                remote(out.at[peer[axis], zz], got2.at[o - 1, zz], slot, peer).start()
            return carry

        lax.fori_loop(lo, hi, step, 0)

    def gather_both(stretch):
        gather(stretch, px, x, rx, sx, rx2, "x", "y", ny, nx, y)
        gather(stretch, py, y, ry, sy, ry2, "y", "x", nx, ny, x)

    small_rows = (taps + 2 + 7) // 8
    flat = sa.shape[0] * sa.shape[1]

    def tap_block(b):
        def step(t, acc):
            base = t * (8 * GROUP)
            h = [hg_v[b, pl.ds(pl.multiple_of(base + 8 * u, 8), 8), :] for u in range(GROUP)]
            acc = list(acc)
            for k in range(taps + 8 * (GROUP - 1)):
                v = gt_v[b, pl.ds(base + (HALO - reach) + k, 8), :]
                for u in range(GROUP):
                    if 0 <= k - 8 * u < taps:
                        acc[k - 8 * u] = acc[k - 8 * u] + h[u] * v
            return tuple(acc)

        acc = lax.fori_loop(
            0, rows // (8 * GROUP), step, tuple(jnp.zeros((8, LANE), F32) for _ in range(taps)))
        acc = list(acc) + [partial[b], partial[blocks + b]]
        lines = [jnp.sum(a, axis=0, keepdims=True) for a in acc]
        lines += [jnp.zeros((1, LANE), F32)] * (small_rows * 8 - len(lines))
        for t in range(small_rows):
            tile = b * small_rows + t
            sa[tile // 2, tile % 2] = jnp.concatenate(lines[t * 8:t * 8 + 8], axis=0)

    for b in range(blocks):
        tap_block(b)
        if b == 1:
            z_step(3, False)
        if b == 2:
            gather_both(0)
        if b == 3:
            z_step(3, True)
    for tile in range(blocks * small_rows, flat):
        sa[tile // 2, tile % 2] = jnp.zeros((8, LANE), F32)
    for o in range(1, plane):
        remote(sa.at[lax.rem(place + o, plane)], ra.at[o - 1], at["a1"] + o - 1, in_plane(o)).start()

    def z_done():
        for direction in (1, -1):
            for leads in (False, True):
                ring(nz // 2 - 1, leads, z, direction).wait_recv()
        for yy in range(ny):
            v = pz[z, yy].astype(F32) + rzr[nz // 2 - 1, yy].astype(F32) + rzl[nz // 2 - 1, yy].astype(F32)
            v = v.astype(BF16)
            for xx in range(nx):
                sz[xx, yy] = v[xx]
        for o in range(1, nx):
            peer = along("x", nx, x, o)
            remote(sz.at[peer["x"]], rz2.at[o - 1], at["z2"] + o - 1, peer).start()

    def small_plane():
        for o in range(1, plane):
            remote(sa.at[0], ra.at[o - 1], at["a1"] + o - 1, in_plane(o)).wait_recv()
        v = sa[place]
        for o in range(plane - 1):
            v = v + ra[o]
        fa[...] = v
        rza[z] = v
        for o in range(1, nz):
            remote(fa, rza.at[z], at["a2"] + z, along("z", nz, z, o)).start()

    def xy_third(stretch, own, me, got, out, last, name, size):
        lo, hi = stretches[stretch]
        for o in range(1, size):
            slot = at[name + "2"] + stretch * (size - 1) + o - 1
            part = got.at[o - 1, pl.ds(0, hi - lo)]
            remote(part, part, slot, other).wait_recv()

        def step(k, carry):
            zz = far(k)
            v = own[me, zz].astype(F32)
            for o in range(size - 1):
                v = v + got[o, zz].astype(F32)
            out[zz] = v.astype(BF16)

            @pl.when(k < nz - 1)
            def _():
                o = lax.rem(zz - z + nz, nz)
                remote(out.at[zz], last.at[o - 1], at[name + "3"] + o - 1, {"z": zz}).start()

            return carry

        lax.fori_loop(lo, hi, step, 0)

    def third_both(stretch):
        xy_third(stretch, sx, y, rx2, tx, rx3, "x", ny)
        xy_third(stretch, sy, x, ry2, ty, ry3, "y", nx)

    def z_third():
        for o in range(1, nx):
            remote(sz.at[0], rz2.at[o - 1], at["z2"] + o - 1, other).wait_recv()
        v = sz[x].astype(F32)
        for o in range(nx - 1):
            v = v + rz2[o].astype(F32)
        tz[...] = v.astype(BF16)
        for o in range(1, ny):
            peer = along("y", ny, y, o)
            remote(tz.at[peer["y"]], rz3.at[o - 1], at["z3"] + o - 1, peer).start()

    def small_line():
        for o in range(1, nz):
            zz = lax.rem(z + o, nz)
            remote(fa, rza.at[zz], at["a2"] + zz, other).wait_recv()
        v = rza[0]
        for zz in range(1, nz):
            v = v + rza[zz]
        fin[...] = v
        ag_a[place] = v
        for o in range(1, plane):
            remote(fin, ag_a.at[place], at["a3"] + o - 1, in_plane(o)).start()

    height_copy.wait_recv()
    for b in range(blocks):
        tail = hh_r[:, lanes(b)].astype(F32)
        hg_v[b, rows:rows + HALO, :] = jnp.where(line == count - 1, 0.0, tail)

    loads["taps"].wait()

    def gated_block(b):
        lines = taps_v[:, lanes(b)].astype(F32)
        spread = [jnp.broadcast_to(lines[j:j + 1, :], (8, LANE)) for j in range(taps)]

        def step(t, carry):
            base = t * (8 * GROUP)
            acc = [[None, None] for _ in range(GROUP)]
            for k in range(taps + 8 * (GROUP - 1)):
                v = hg_v[b, pl.ds(base + k, 8), :]
                for u in range(GROUP):
                    j = reach + 8 * u - k
                    if 0 <= j < taps:
                        term = spread[j] * v
                        old = acc[u][k % 2]
                        acc[u][k % 2] = term if old is None else old + term
            for u in range(0, GROUP, 2):
                r = pl.ds(pl.multiple_of(base + 8 * u, 16), 16)
                g = jnp.concatenate([acc[w][0] + acc[w][1] for w in (u, u + 1)], axis=0)
                s = sg_v[r, lanes(b)]
                gs = g * s
                gv_v[r, lanes(b)] = gs.astype(BF16)
                gg_v[r, lanes(b)] = (gs * cv_v[r, lanes(b)].astype(F32) * (1.0 - s)).astype(BF16)
            return carry

        lax.fori_loop(0, rows // (8 * GROUP), step, 0)

    for b in range(blocks):
        gated_block(b)
        if b == 0:
            gather_both(1)
        if b == 1:
            z_done()
            third_both(0)
        if b == 2:
            small_plane()
        if b == 3:
            third_both(1)
            z_third()
        if b == 5:
            small_line()

    for buf, own, last, name in ((0, tx, rx3, "x3"), (1, ty, ry3, "y3")):
        for o in range(1, nz):
            remote(own.at[0], last.at[o - 1], at[name] + o - 1, other).wait_recv()
        v = own[z].astype(F32)
        for o in range(nz - 1):
            v = v + last[o].astype(F32)
        proj_v[:, buf * third:(buf + 1) * third] = v
    for o in range(1, ny):
        remote(tz.at[0], rz3.at[o - 1], at["z3"] + o - 1, other).wait_recv()
    v = tz[y].astype(F32)
    for o in range(ny - 1):
        v = v + rz3[o].astype(F32)
    proj_v[:, 2 * third:] = v

    for o in range(1, plane):
        p = lax.rem(place - o + plane, plane)
        remote(fin, ag_a.at[p], at["a3"] + o - 1, other).wait_recv()
    for b in range(blocks):
        for t in range(small_rows):
            tile = b * small_rows + t
            v = ag_a[tile // 2, tile % 2]
            keep = min(8, taps - t * 8)
            if keep > 0:
                taps_o[t * 8:t * 8 + keep, lanes(b)] = v[0:keep]
            for row, out in ((taps, gain_o), (taps + 1, shift_o)):
                if row // 8 == t:
                    out[lanes(b)] = v[row % 8:row % 8 + 1].reshape(LANE)

    stat_copy.wait_send()
    gated_copy.wait_send()
    sums_copy.wait_send()
    height_copy.wait_send()
    for stretch, (lo, hi) in enumerate(stretches):
        some = pl.ds(0, hi - lo)
        for o in range(nx - 1):
            remote(px.at[0, some], rx.at[o, some], at["x1"] + stretch * (nx - 1) + o, other).wait_send()
            remote(sy.at[0, some], ry2.at[o, some], at["y2"] + stretch * (nx - 1) + o, other).wait_send()
        for o in range(ny - 1):
            remote(py.at[0, some], ry.at[o, some], at["y1"] + stretch * (ny - 1) + o, other).wait_send()
            remote(sx.at[0, some], rx2.at[o, some], at["x2"] + stretch * (ny - 1) + o, other).wait_send()
    for o in range(nx - 1):
        remote(sz.at[0], rz2.at[o], at["z2"] + o, other).wait_send()
    for o in range(ny - 1):
        remote(tz.at[0], rz3.at[o], at["z3"] + o, other).wait_send()
    for o in range(nz - 1):
        remote(tx.at[0], rx3.at[o], at["x3"] + o, other).wait_send()
        remote(ty.at[0], ry3.at[o], at["y3"] + o, other).wait_send()
    for step in range(nz // 2):
        for direction in (1, -1):
            ring(step, True, z, direction).wait_send()
            if step > 0:
                ring(step, False, z, direction).wait_send()
    for o in range(plane - 1):
        remote(sa.at[0], ra.at[o], at["a1"] + o, other).wait_send()
        remote(fin, ag_a.at[0], at["a3"] + o, other).wait_send()
    for o in range(1, nz):
        remote(fa, rza.at[z], at["a2"] + z, other).wait_send()


def local(conv_value, conv_gate, conv_out, conv_taps, norm_gain, norm_shift, proj_weight, out_grad):
    nz, ny, nx = (lax.axis_size(a) for a in SP)
    rows, chan = conv_value.shape
    depth = out_grad.shape[1]
    taps = conv_taps.shape[0]
    blocks = chan // LANE
    third = chan // 3
    plane = ny * nx
    slots, _ = layout(nz, ny, nx)
    vm = pltpu.VMEM
    small_rows = (taps + 2 + 7) // 8 * 8
    per = -(-blocks * small_rows // 8 // plane)
    scratch = [
        vm((rows, chan), BF16), vm((rows, depth), BF16), vm((depth, chan), BF16), vm((rows, chan), BF16),
        vm((rows, chan), BF16), vm((taps, chan), BF16), vm((chan,), F32), vm((chan,), F32),
        vm((2, rows, LANE), F32), vm((2, rows, LANE), F32), vm((2, rows, LANE), F32), vm((2, rows, LANE), F32),
        vm((rows, LANE), F32), vm((rows, chan), F32), vm((blocks, rows + HALO, LANE), F32), vm((rows, chan), F32),
        vm((rows, chan), F32), vm((rows, chan), BF16), vm((rows, chan), F32), vm((blocks, rows + HALO, LANE), F32),
        vm((HALO, chan), BF16), vm((HALO, chan), BF16), vm((HALO, chan), BF16), vm((HALO, chan), BF16),
        vm((nx, nz, ny, 16, third), BF16), vm((ny, nz, nx, 16, third), BF16), vm((nz, ny, nx, 16, third), BF16),
        vm((nx - 1, nz, ny, 16, third), BF16), vm((ny - 1, nz, nx, 16, third), BF16),
        vm((nz // 2, ny, nx, 16, third), BF16), vm((nz // 2, ny, nx, 16, third), BF16),
        vm((ny, nz, 16, third), BF16), vm((nx, nz, 16, third), BF16),
        vm((ny - 1, nz, 16, third), BF16), vm((nx - 1, nz, 16, third), BF16),
        vm((nz, 16, third), BF16), vm((nz, 16, third), BF16),
        vm((nz - 1, 16, third), BF16), vm((nz - 1, 16, third), BF16),
        vm((nx, ny, 16, third), BF16), vm((nx - 1, ny, 16, third), BF16),
        vm((ny, 16, third), BF16), vm((ny - 1, 16, third), BF16),
        vm((plane, per, 8, LANE), F32), vm((plane - 1, per, 8, LANE), F32), vm((per, 8, LANE), F32),
        vm((nz, per, 8, LANE), F32), vm((per, 8, LANE), F32), vm((plane, per, 8, LANE), F32),
        pltpu.SemaphoreType.DMA((8,)),
        pltpu.SemaphoreType.DMA((slots.used,)), pltpu.SemaphoreType.DMA((slots.used,)),
    ]
    anywhere = pl.BlockSpec(memory_space=pl.ANY)
    shapes = (
        ((rows, chan), BF16), ((rows, chan), BF16), ((taps, chan), F32), ((chan,), F32), ((chan,), F32), ((16, chan), F32),
    )
    held = pl.BlockSpec(memory_space=pltpu.VMEM)
    results = pl.pallas_call(
        functools.partial(kernel, (nz, ny, nx, rows, chan, depth, taps)),
        out_shape=tuple(pltpu.VMEM(*s) for s in shapes),
        in_specs=[anywhere] * 8,
        out_specs=(held,) * 6,
        scratch_shapes=scratch,
        compiler_params=pltpu.CompilerParams(
            collective_id=0, has_side_effects=True, vmem_limit_bytes=36 * 1024 * 1024),
        name="module_backward",
    )(*(pltpu.with_memory_space_constraint(a, pltpu.HBM) for a in (
        conv_value, conv_gate, conv_out, conv_taps, norm_gain, norm_shift, proj_weight, out_grad)))
    return pl.pallas_call(
        write_out,
        out_shape=tuple(jax.ShapeDtypeStruct(*s) for s in shapes),
        in_specs=[held] * 6,
        out_specs=(anywhere,) * 6,
        scratch_shapes=[pltpu.SemaphoreType.DMA((6,))],
        name="write_out",
    )(*(pltpu.with_memory_space_constraint(a, pltpu.VMEM) for a in results))


def write_out(*refs):
    sem = refs[12]
    copies = [pltpu.make_async_copy(refs[i], refs[6 + i], sem.at[i]) for i in range(6)]
    for c in copies:
        c.start()
    for c in copies:
        c.wait()


def solution(mesh):
    split = Mesh(mesh.devices.reshape(8, 4, 4, mesh.shape["tp"]), (*SP, "tp"))
    placed = (
        P(SP, "tp"), P(SP, "tp"), P(SP, "tp"), P(None, "tp"), P("tp"), P("tp"), P(None, "tp"), P(SP, None),
    )
    return jax.shard_map(
        local,
        mesh=split,
        in_specs=placed,
        out_specs=(P(SP, "tp"), P(SP, "tp"), P(None, "tp"), P("tp"), P("tp"), P(SP, "tp")),
        check_vma=False,
    )
```

```python
import functools

import jax
import jax.numpy as jnp
from jax import lax
from jax.experimental import pallas as pl
from jax.experimental.pallas import tpu as pltpu
from jax.sharding import Mesh
from jax.sharding import PartitionSpec as P

MESH = pl.DeviceIdType.MESH
F32 = jnp.float32
BF16 = jnp.bfloat16
SP = ("z", "y", "x")
EPS = 1e-05
HALO = 32
LANE = 128
TILE = 32
GROUP = 8
FIRST = 128
FAR, NEAR, SUM = range(3)


class Slots:
    def __init__(self):
        self.used = 0

    def take(self, count):
        first = self.used
        self.used += count
        return first


def layout(nz, ny, nx):
    slots = Slots()
    plane = ny * nx
    return slots, {
        "stat": slots.take(1),
        "sums": slots.take(1),
        "gated": slots.take(1),
        "height": slots.take(1),
        "far": slots.take(2),
        "near": slots.take(2),
        "second": slots.take(2),
        "last": slots.take(1),
        "leads": slots.take(nz // 2),
        "trails": slots.take(nz // 2),
        "z2": slots.take(1),
        "z3": slots.take(1),
        "a1": slots.take(1),
        "a2": slots.take(1),
        "a3": slots.take(1),
    }


def kernel(sizes, *refs):
    nz, ny, nx, rows, chan, depth, taps = sizes
    cv_h, cg_h, co_h, taps_h, gain_h, shift_h, w_h, og_h, gv_v, gg_v, taps_o, gain_o, shift_o, proj_v = refs[:14]
    (co_v, og_v, ogt_v, w_v, cv_v, cg_v, taps_v, gain_v, shift_v, st_s, st_r, s2_s, s2_r, iv_v, sg_v, gt_v, nm_v, ds_v,
     act_v, ag_v, hg_v, gh_s, gh_r, hh_s, hh_r, pxy, pz, fxy, rxy, rzr, rzl, sxy, rxy2, txy, rxy3,
     sz, rz2, tz, rz3, stage, sa, ra, fa, rza, fin, ag_a, in_sem, ssem, rsem) = refs[14:]
    blocks = chan // LANE
    total = 2 * chan
    reach = taps - 1
    plane = ny * nx
    per = stage.shape[0] // plane
    px, fx, rx, sx, rx2, tx, rx3 = (a.at[0] for a in (pxy, fxy, rxy, sxy, rxy2, txy, rxy3))
    py, fy, ry, sy, ry2, ty, ry3 = (a.at[1] for a in (pxy, fxy, rxy, sxy, rxy2, txy, rxy3))
    _, at = layout(nz, ny, nx)
    z, y, x, core = (lax.axis_index(a) for a in ("z", "y", "x", "tp"))
    place = y * nx + x
    line = z * plane + place
    count = nz * plane

    def where(index):
        return {"z": lax.div(index, plane), "y": lax.rem(lax.div(index, nx), ny), "x": lax.rem(index, nx)}

    after = where(lax.rem(line + 1, count))
    before = where(lax.rem(line + count - 1, count))
    other = {"tp": 1 - core}

    def along(axis, size, me, step):
        return {axis: lax.rem(me + step + size, size)}

    def in_plane(step):
        p = lax.rem(place + step, plane)
        return {"y": lax.div(p, nx), "x": lax.rem(p, nx)}

    def remote(src, dst, slot, target):
        return pltpu.make_async_remote_copy(
            src_ref=src, dst_ref=dst, send_sem=ssem.at[slot], recv_sem=rsem.at[slot],
            device_id=target, device_id_type=MESH)

    loads = {}
    for slot, (name, src, dst) in enumerate((
            ("co", co_h, co_v), ("gain", gain_h, gain_v), ("shift", shift_h, shift_v), ("cg", cg_h, cg_v),
            ("cv", cv_h, cv_v), ("og", og_h, og_v), ("w", w_h, w_v), ("taps", taps_h, taps_v))):
        loads[name] = pltpu.make_async_copy(src, dst, in_sem.at[slot])
        loads[name].start()

    barrier = pltpu.get_barrier_semaphore()
    peers = [other, after, before]
    peers += [in_plane(o) for o in range(1, plane)]
    peers += [along("z", nz, z, o) for o in range(1, nz)]
    for peer in peers:
        pl.semaphore_signal(barrier, inc=1, device_id=peer, device_id_type=MESH)

    def lanes(b):
        return slice(b * LANE, (b + 1) * LANE)

    loads["co"].wait()

    wide = rows // 2

    def means(i, carry):
        for u in range(wide // 64):
            r = pl.ds(pl.multiple_of(i * wide + u * 64, 64), 64)
            m = jnp.sum(co_v[r, :].astype(F32), axis=1, keepdims=True) * (1.0 / chan)
            st_s[0, r, :] = jnp.broadcast_to(m, (64, LANE))
        return carry

    lax.fori_loop(0, 2, means, 0)

    def spreads(i, carry):
        for u in range(wide // 64):
            r = pl.ds(pl.multiple_of(i * wide + u * 64, 64), 64)
            m = st_s[0, r, :]
            q = jnp.zeros((64, LANE), F32)
            for b in range(blocks):
                d = co_v[r, lanes(b)].astype(F32) - m
                q = q + d * d
            st_s[1, r, :] = jnp.broadcast_to(jnp.sum(q, axis=1, keepdims=True), (64, LANE))
        return carry

    lax.fori_loop(0, 2, spreads, 0)

    pl.semaphore_wait(barrier, len(peers))
    stat_copy = remote(st_s, st_r, at["stat"], other)
    stat_copy.start()
    loads["cg"].wait()
    loads["cv"].wait()

    def gates(i, carry):
        r = pl.ds(pl.multiple_of(i * TILE, TILE), TILE)
        up = pl.ds(pl.multiple_of(i * TILE + HALO, TILE), TILE)
        for b in range(blocks):
            s = 0.5 * jnp.tanh(0.5 * cg_v[r, lanes(b)].astype(F32)) + 0.5
            sg_v[r, lanes(b)] = s
            gt_v[b, up, :] = (cv_v[r, lanes(b)].astype(F32) * s).astype(BF16).astype(F32)
        return carry

    lax.fori_loop(0, rows // TILE, gates, 0)
    for b in range(blocks):
        gh_s[:, lanes(b)] = gt_v[b, rows:rows + HALO, :].astype(BF16)

    gated_copy = remote(gh_s, gh_r, at["gated"], after)

    @pl.when(line < count - 1)
    def _():
        gated_copy.start()


    loads["og"].wait()

    span = plane * 16

    def far(k):
        away = nz // 2 - lax.div(k + 1, 2)
        return lax.rem(z + (2 * lax.rem(k, 2) - 1) * away + nz, nz)

    def turn(k, carry):
        cols = pl.ds(pl.multiple_of(far(k) * span, span), span)
        ogt_v[pl.ds(pl.multiple_of(k * span, span), span), :] = og_v[:, cols].T
        return carry

    lax.fori_loop(0, nz, turn, 0)
    loads["w"].wait()
    ag_v[0:FIRST, :] = jnp.dot(og_v[0:FIRST, :], w_v[...], preferred_element_type=F32)
    loads["gain"].wait()
    loads["shift"].wait()
    stat_copy.wait_recv()

    def norm(i, carry):
        r = pl.ds(pl.multiple_of(i * TILE, TILE), TILE)
        m1, m2 = st_s[0, r, :], st_r[0, r, :]
        gap = m1 - m2
        mean = 0.5 * (m1 + m2)
        inv = lax.rsqrt((st_s[1, r, :] + st_r[1, r, :] + gap * gap * (chan / 2)) * (1.0 / total) + EPS)
        iv_v[r, :] = inv
        for b in range(blocks):
            n = (co_v[r, lanes(b)].astype(F32) - mean) * inv
            s = n * gain_v[lanes(b)].reshape(1, LANE) + shift_v[lanes(b)].reshape(1, LANE)
            sig = 0.5 * jnp.tanh(0.5 * s) + 0.5
            a = s * sig
            act_v[r, lanes(b)] = a.astype(BF16)
            nm_v[r, lanes(b)] = n
            ds_v[r, lanes(b)] = sig + a * (1.0 - sig)
        return carry

    lax.fori_loop(0, rows // TILE, norm, 0)

    third = chan // 3
    half = ny // 2
    stretches = ((0, nz // 2), (nz // 2, nz))
    upper, lower = pl.ds(0, half), pl.ds(half, half)

    def ring(step, leads, src_z, direction):
        buf = rzr if direction > 0 else rzl
        part = upper if leads == (direction > 0) else lower
        slot = at["leads" if leads else "trails"] + step
        return remote(pz.at[src_z, part], buf.at[step, part], slot, along("z", nz, z, direction))

    rings = {"x": (px, fx, rx, x), "y": (py, fy, ry, y)}

    def hop(axis, stretch, kind, direction, lines):
        wide, far_got, got, me = rings[axis]
        d = 0 if direction > 0 else 1
        mine, rest = (upper, lower) if direction > 0 else (lower, upper)
        slot = at["far" if kind == FAR else "near"] + stretch
        peer = along(axis, 4, me, direction)
        if kind == FAR:
            return remote(wide.at[lax.rem(me + 2, 4), lines, mine], far_got.at[d, lines], slot, peer)
        part = rest if kind == NEAR else mine
        return remote(wide.at[peer[axis], lines, part], got.at[d, lines, part], slot, peer)

    def relay(stretch):
        lo, hi = stretches[stretch]
        part = fxy.at[:, :, pl.ds(0, hi - lo)]
        remote(part, part, at["far"] + stretch, other).wait_recv()
        for axis in ("x", "y"):
            wide, far_got, _, me = rings[axis]
            for direction in (1, -1):
                d, first = (0, 0) if direction > 0 else (1, half)
                dest = lax.rem(me + direction + 4, 4)

                def step(k, carry):
                    for w in range(half):
                        v = wide[dest, k, first + w].astype(F32) + far_got[d, k, w].astype(F32)
                        wide[dest, k, first + w] = v.astype(BF16)
                    return carry

                lax.fori_loop(lo, hi, step, 0)
                hop(axis, stretch, SUM, direction, pl.ds(lo, hi - lo)).start()

    def ring_wait(step, leads):
        return remote(pz.at[0], pz.at[0], at["leads" if leads else "trails"] + step, other)

    def project(stretch):
        def step(i, carry):
            lines = pl.ds(pl.multiple_of(i * 2 * span, span), 2 * span)
            both = jnp.dot(ogt_v[lines, :], act_v[...], preferred_element_type=F32)
            for u in range(2):
                k = 2 * i + u
                zz = far(k)
                block = both[u * span:(u + 1) * span].astype(BF16)
                for yy in range(ny):
                    for xx in range(nx):
                        part = slice((yy * nx + xx) * 16, (yy * nx + xx) * 16 + 16)
                        px[xx, k, yy] = block[part, 0:third]
                        py[yy, k, xx] = block[part, third:2 * third]
                        pz[zz, yy, xx] = block[part, 2 * third:]
            if stretch == 0:
                @pl.when(i == 0)
                def _():
                    for direction in (1, -1):
                        ring(0, True, far(0), direction).start()
                    ring(1, False, far(1), 1).start()

                @pl.when(i == 1)
                def _():
                    ring(1, False, far(2), -1).start()

            return carry

        lo, hi = stretches[stretch]
        lax.fori_loop(lo // 2, hi // 2, step, 0)
        for kind in (FAR, NEAR):
            for axis in ("x", "y"):
                for direction in (1, -1):
                    hop(axis, stretch, kind, direction, pl.ds(lo, hi - lo)).start()

    def z_step(step, leads):
        ring_wait(step - 1, leads).wait_recv()
        for direction in (1, -1):
            dest = lax.rem(z + direction * (nz // 2 - step) + nz, nz)
            buf = rzr if direction > 0 else rzl
            for yy in (range(half) if leads == (direction > 0) else range(half, ny)):
                pz[dest, yy] = (pz[dest, yy].astype(F32) + buf[step - 1, yy].astype(F32)).astype(BF16)
            ring(step, leads, dest, direction).start()

    project(0)

    ag_v[FIRST:, :] = jnp.dot(og_v[FIRST:, :], w_v[...], preferred_element_type=F32)

    def grads(i, carry):
        r = pl.ds(pl.multiple_of(i * TILE, TILE), TILE)
        carry = list(carry)
        row_sum = jnp.zeros((TILE, LANE), F32)
        row_dot = jnp.zeros((TILE, LANE), F32)
        for b in range(blocks):
            g = ag_v[r, lanes(b)] * ds_v[r, lanes(b)]
            n = nm_v[r, lanes(b)]
            gn = g * n
            carry[b] = carry[b] + jnp.sum(gn.reshape(TILE // 8, 8, LANE), axis=0)
            carry[blocks + b] = carry[blocks + b] + jnp.sum(g.reshape(TILE // 8, 8, LANE), axis=0)
            gain = gain_v[lanes(b)].reshape(1, LANE)
            s = g * gain
            ag_v[r, lanes(b)] = s
            row_sum = row_sum + s
            row_dot = row_dot + gn * gain
        s2_s[0, r, :] = row_sum
        s2_s[1, r, :] = row_dot
        return tuple(carry)

    partial = lax.fori_loop(0, rows // TILE, grads, tuple(jnp.zeros((8, LANE), F32) for _ in range(2 * blocks)))

    def channel_sums(i, carry):
        for u in range(wide // 64):
            r = pl.ds(pl.multiple_of(i * wide + u * 64, 64), 64)
            for w in range(2):
                v = jnp.sum(s2_s[w, r, :], axis=1, keepdims=True)
                s2_s[w, r, :] = jnp.broadcast_to(v, (64, LANE))
        return carry

    lax.fori_loop(0, 2, channel_sums, 0)
    sums_copy = remote(s2_s, s2_r, at["sums"], other)
    sums_copy.start()

    project(1)
    relay(0)
    z_step(1, True)

    @pl.when(line > 0)
    def _():
        gated_copy.wait_recv()

    for b in range(blocks):
        head = gh_r[:, lanes(b)].astype(F32)
        gt_v[b, 0:HALO, :] = jnp.where(line == 0, 0.0, head)

    sums_copy.wait_recv()

    def height(i, carry):
        r = pl.ds(pl.multiple_of(i * TILE, TILE), TILE)
        sums = (s2_s[0, r, :] + s2_r[0, r, :]) * (1.0 / total)
        dots = (s2_s[1, r, :] + s2_r[1, r, :]) * (1.0 / total)
        inv = iv_v[r, :]
        for b in range(blocks):
            hg_v[b, r, :] = inv * (ag_v[r, lanes(b)] - sums - nm_v[r, lanes(b)] * dots)
        return carry

    lax.fori_loop(0, rows // TILE, height, 0)
    for b in range(blocks):
        hh_s[:, lanes(b)] = hg_v[b, 0:HALO, :].astype(BF16)
    height_copy = remote(hh_s, hh_r, at["height"], before)

    @pl.when(line > 0)
    def _():
        height_copy.start()


    def gather(stretch, wide, me, got, out, got2, axis, size, own_me):
        lo, hi = stretches[stretch]

        def step(k, carry):
            v = (wide[me, k].astype(F32) + got[0, k].astype(F32) + got[1, k].astype(F32)).astype(BF16)
            for w in range(size):
                out[w, k] = v[w]
            return carry

        lax.fori_loop(lo, hi, step, 0)
        some = pl.ds(lo, hi - lo)
        for o in range(1, size):
            peer = along(axis, size, own_me, o)
            remote(out.at[peer[axis], some], got2.at[o - 1, some], at["second"] + stretch, peer).start()

    def gather_both(stretch):
        lo, hi = stretches[stretch]
        part = rxy.at[:, :, pl.ds(0, hi - lo)]
        remote(part, part, at["near"] + stretch, other).wait_recv()
        gather(stretch, px, x, rx, sx, rx2, "y", ny, y)
        gather(stretch, py, y, ry, sy, ry2, "x", nx, x)

    used = blocks * (taps + 2)
    stage[used:, :] = jnp.zeros((stage.shape[0] - used, LANE), F32)

    def tap_block(b):
        def step(t, acc):
            base = t * (8 * GROUP)
            h = [hg_v[b, pl.ds(pl.multiple_of(base + 8 * u, 8), 8), :] for u in range(GROUP)]
            acc = list(acc)
            for k in range(taps + 8 * (GROUP - 1)):
                v = gt_v[b, pl.ds(base + (HALO - reach) + k, 8), :]
                for u in range(GROUP):
                    if 0 <= k - 8 * u < taps:
                        acc[k - 8 * u] = acc[k - 8 * u] + h[u] * v
            return tuple(acc)

        acc = lax.fori_loop(
            0, rows // (8 * GROUP), step, tuple(jnp.zeros((8, LANE), F32) for _ in range(taps)))
        acc = list(acc) + [partial[b], partial[blocks + b]]
        for j, a in enumerate(acc):
            row = b * (taps + 2) + j
            stage[row:row + 1, :] = jnp.sum(a, axis=0, keepdims=True)

    for b in range(blocks):
        tap_block(b)
        if b == 0:
            z_step(2, False)
        if b == 3:
            z_step(2, True)
            relay(1)
    for p in range(plane):
        sa[p] = stage[p * per:(p + 1) * per, :].astype(BF16)
    for o in range(1, plane):
        remote(sa.at[lax.rem(place + o, plane)], ra.at[o - 1], at["a1"], in_plane(o)).start()

    def z_done():
        for leads in (False, True):
            ring_wait(nz // 2 - 1, leads).wait_recv()
        for yy in range(ny):
            v = pz[z, yy].astype(F32) + rzr[nz // 2 - 1, yy].astype(F32) + rzl[nz // 2 - 1, yy].astype(F32)
            v = v.astype(BF16)
            for xx in range(nx):
                sz[xx, yy] = v[xx]
        for o in range(1, nx):
            peer = along("x", nx, x, o)
            remote(sz.at[peer["x"]], rz2.at[o - 1], at["z2"], peer).start()

    def small_plane():
        remote(ra, ra, at["a1"], other).wait_recv()
        v = stage[pl.ds(pl.multiple_of(place * per, 8), per), :]
        for o in range(plane - 1):
            v = v + ra[o].astype(F32)
        fa[...] = v
        rza[z] = v
        for o in range(1, nz):
            remote(fa, rza.at[z], at["a2"], along("z", nz, z, o)).start()

    def xy_third(stretch, own, me, got, out, last, size):
        lo, hi = stretches[stretch]
        def step(k, carry):
            zz = far(k)
            v = own[me, k].astype(F32)
            for o in range(size - 1):
                v = v + got[o, k].astype(F32)
            out[k] = v.astype(BF16)

            @pl.when(k < nz - 1)
            def _():
                o = lax.rem(zz - z + nz, nz)
                remote(out.at[k], last.at[o - 1], at["last"], {"z": zz}).start()

            return carry

        lax.fori_loop(lo, hi, step, 0)

    def third_both(stretch):
        lo, hi = stretches[stretch]
        part = rxy2.at[:, :, pl.ds(0, hi - lo)]
        remote(part, part, at["second"] + stretch, other).wait_recv()
        xy_third(stretch, sx, y, rx2, tx, rx3, ny)
        xy_third(stretch, sy, x, ry2, ty, ry3, nx)

    def z_third():
        remote(rz2, rz2, at["z2"], other).wait_recv()
        v = sz[x].astype(F32)
        for o in range(nx - 1):
            v = v + rz2[o].astype(F32)
        tz[...] = v.astype(BF16)
        for o in range(1, ny):
            peer = along("y", ny, y, o)
            remote(tz.at[peer["y"]], rz3.at[o - 1], at["z3"], peer).start()

    def small_line():
        rest = rza.at[pl.ds(0, nz - 1)]
        remote(rest, rest, at["a2"], other).wait_recv()
        v = rza[0]
        for zz in range(1, nz):
            v = v + rza[zz]
        fin[...] = v
        ag_a[place] = v
        for o in range(1, plane):
            remote(fin, ag_a.at[place], at["a3"], in_plane(o)).start()

    z_step(3, False)
    gather_both(0)

    @pl.when(line < count - 1)
    def _():
        height_copy.wait_recv()

    for b in range(blocks):
        tail = hh_r[:, lanes(b)].astype(F32)
        hg_v[b, rows:rows + HALO, :] = jnp.where(line == count - 1, 0.0, tail)

    loads["taps"].wait()

    def gated_block(b):
        lines = taps_v[:, lanes(b)].astype(F32)
        spread = [jnp.broadcast_to(lines[j:j + 1, :], (8, LANE)) for j in range(taps)]

        def step(t, carry):
            base = t * (8 * GROUP)
            acc = [None] * GROUP
            for k in range(taps + 8 * (GROUP - 1)):
                v = hg_v[b, pl.ds(base + k, 8), :]
                for u in range(GROUP):
                    j = reach + 8 * u - k
                    if 0 <= j < taps:
                        term = spread[j] * v
                        acc[u] = term if acc[u] is None else acc[u] + term
            for u in range(0, GROUP, 2):
                r = pl.ds(pl.multiple_of(base + 8 * u, 16), 16)
                g = jnp.concatenate(acc[u:u + 2], axis=0)
                s = sg_v[r, lanes(b)]
                gs = g * s
                gv_v[r, lanes(b)] = gs.astype(BF16)
                gg_v[r, lanes(b)] = (gs * cv_v[r, lanes(b)].astype(F32) * (1.0 - s)).astype(BF16)
            return carry

        lax.fori_loop(0, rows // (8 * GROUP), step, 0)

    for b in range(blocks):
        gated_block(b)
        if b == 1:
            z_step(3, True)
            gather_both(1)
        if b == 3:
            small_plane()
        if b == 4:
            third_both(0)
        if b == 5:
            third_both(1)
            z_done()
            small_line()
            z_third()

    remote(rxy3, rxy3, at["last"], other).wait_recv()
    for buf, own, last in ((0, tx, rx3), (1, ty, ry3)):
        v = own[nz - 1].astype(F32)
        for o in range(nz - 1):
            v = v + last[o].astype(F32)
        proj_v[:, buf * third:(buf + 1) * third] = v
    remote(rz3, rz3, at["z3"], other).wait_recv()
    v = tz[y].astype(F32)
    for o in range(ny - 1):
        v = v + rz3[o].astype(F32)
    proj_v[:, 2 * third:] = v

    rest = ag_a.at[pl.ds(0, plane - 1)]
    remote(rest, rest, at["a3"], other).wait_recv()
    for b in range(blocks):
        for j in range(taps + 2):
            row = b * (taps + 2) + j
            v = ag_a[row // per, row % per:row % per + 1, :]
            if j < taps:
                taps_o[j:j + 1, lanes(b)] = v
            else:
                (gain_o if j == taps else shift_o)[lanes(b)] = v.reshape(LANE)

    stat_copy.wait_send()

    @pl.when(line < count - 1)
    def _():
        gated_copy.wait_send()

    sums_copy.wait_send()

    @pl.when(line > 0)
    def _():
        height_copy.wait_send()

    for stretch, (lo, hi) in enumerate(stretches):
        some = pl.ds(0, hi - lo)
        for name, buf in (("far", fxy), ("near", rxy), ("second", rxy2)):
            part = buf.at[:, :, some]
            remote(part, part, at[name] + stretch, other).wait_send()
    for step in range(nz // 2):
        ring_wait(step, True).wait_send()
        if step > 0:
            ring_wait(step, False).wait_send()
    for name, part in (("last", rxy3), ("z2", rz2), ("z3", rz3), ("a1", ra), ("a2", rza.at[pl.ds(0, nz - 1)]), ("a3", rest)):
        remote(part, part, at[name], other).wait_send()


def local(conv_value, conv_gate, conv_out, conv_taps, norm_gain, norm_shift, proj_weight, out_grad):
    nz, ny, nx = (lax.axis_size(a) for a in SP)
    rows, chan = conv_value.shape
    depth = out_grad.shape[1]
    taps = conv_taps.shape[0]
    blocks = chan // LANE
    third = chan // 3
    plane = ny * nx
    slots, _ = layout(nz, ny, nx)
    vm = pltpu.VMEM
    per = -(-(blocks * (taps + 2)) // (16 * plane)) * 16
    scratch = [
        vm((rows, chan), BF16), vm((rows, depth), BF16), vm((depth, rows), BF16), vm((depth, chan), BF16), vm((rows, chan), BF16),
        vm((rows, chan), BF16), vm((taps, chan), BF16), vm((chan,), F32), vm((chan,), F32),
        vm((2, rows, LANE), F32), vm((2, rows, LANE), F32), vm((2, rows, LANE), F32), vm((2, rows, LANE), F32),
        vm((rows, LANE), F32), vm((rows, chan), F32), vm((blocks, rows + HALO, LANE), F32), vm((rows, chan), F32),
        vm((rows, chan), F32), vm((rows, chan), BF16), vm((rows, chan), F32), vm((blocks, rows + HALO, LANE), F32),
        vm((HALO, chan), BF16), vm((HALO, chan), BF16), vm((HALO, chan), BF16), vm((HALO, chan), BF16),
        vm((2, 4, nz, 4, 16, third), BF16), vm((nz, 4, 4, 16, third), BF16),
        vm((2, 2, nz, 2, 16, third), BF16), vm((2, 2, nz, 4, 16, third), BF16),
        vm((nz // 2, 4, 4, 16, third), BF16), vm((nz // 2, 4, 4, 16, third), BF16),
        vm((2, 4, nz, 16, third), BF16), vm((2, 3, nz, 16, third), BF16),
        vm((2, nz, 16, third), BF16), vm((2, nz - 1, 16, third), BF16),
        vm((nx, ny, 16, third), BF16), vm((nx - 1, ny, 16, third), BF16),
        vm((ny, 16, third), BF16), vm((ny - 1, 16, third), BF16),
        vm((plane * per, LANE), F32), vm((plane, per, LANE), BF16), vm((plane - 1, per, LANE), BF16), vm((per, LANE), F32),
        vm((nz, per, LANE), F32), vm((per, LANE), F32), vm((plane, per, LANE), F32),
        pltpu.SemaphoreType.DMA((8,)),
        pltpu.SemaphoreType.DMA((slots.used,)), pltpu.SemaphoreType.DMA((slots.used,)),
    ]
    anywhere = pl.BlockSpec(memory_space=pl.ANY)
    shapes = (
        ((rows, chan), BF16), ((rows, chan), BF16), ((taps, chan), F32), ((chan,), F32), ((chan,), F32), ((16, chan), F32),
    )
    held = pl.BlockSpec(memory_space=pltpu.VMEM)
    results = pl.pallas_call(
        functools.partial(kernel, (nz, ny, nx, rows, chan, depth, taps)),
        out_shape=tuple(pltpu.VMEM(*s) for s in shapes),
        in_specs=[anywhere] * 8,
        out_specs=(held,) * 6,
        scratch_shapes=scratch,
        compiler_params=pltpu.CompilerParams(
            collective_id=0, has_side_effects=True, vmem_limit_bytes=36 * 1024 * 1024),
        name="module_backward",
    )(*(pltpu.with_memory_space_constraint(a, pltpu.HBM) for a in (
        conv_value, conv_gate, conv_out, conv_taps, norm_gain, norm_shift, proj_weight, out_grad)))
    return pl.pallas_call(
        write_out,
        out_shape=tuple(jax.ShapeDtypeStruct(*s) for s in shapes),
        in_specs=[held] * 6,
        out_specs=(anywhere,) * 6,
        scratch_shapes=[pltpu.SemaphoreType.DMA((6,))],
        name="write_out",
    )(*(pltpu.with_memory_space_constraint(a, pltpu.VMEM) for a in results))


def write_out(*refs):
    sem = refs[12]
    copies = [pltpu.make_async_copy(refs[i], refs[6 + i], sem.at[i]) for i in range(6)]
    for c in copies:
        c.start()
    for c in copies:
        c.wait()


def solution(mesh):
    split = Mesh(mesh.devices.reshape(8, 4, 4, mesh.shape["tp"]), (*SP, "tp"))
    placed = (
        P(SP, "tp"), P(SP, "tp"), P(SP, "tp"), P(None, "tp"), P("tp"), P("tp"), P(None, "tp"), P(SP, None),
    )
    return jax.shard_map(
        local,
        mesh=split,
        in_specs=placed,
        out_specs=(P(SP, "tp"), P(SP, "tp"), P(None, "tp"), P("tp"), P("tp"), P(SP, "tp")),
        check_vma=False,
    )
```

```python
import functools

import jax
import jax.numpy as jnp
from jax import lax
from jax.experimental import pallas as pl
from jax.experimental.pallas import tpu as pltpu
from jax.sharding import Mesh
from jax.sharding import PartitionSpec as P

MESH = pl.DeviceIdType.MESH
F32 = jnp.float32
BF16 = jnp.bfloat16
SP = ("z", "y", "x")
EPS = 1e-05
HALO = 32
LANE = 128
TILE = 32
GROUP = 8
FIRST = 128
FAR, NEAR, SUM = range(3)


class Slots:
    def __init__(self):
        self.used = 0

    def take(self, count):
        first = self.used
        self.used += count
        return first


def layout(nz, ny, nx):
    slots = Slots()
    plane = ny * nx
    return slots, {
        "stat": slots.take(1),
        "sums": slots.take(1),
        "gated": slots.take(1),
        "height": slots.take(1),
        "far": slots.take(2),
        "near": slots.take(2),
        "second": slots.take(2),
        "last": slots.take(1),
        "leads": slots.take(nz // 2),
        "trails": slots.take(nz // 2),
        "z2": slots.take(1),
        "z3": slots.take(1),
        "a1": slots.take(1),
        "a2": slots.take(1),
        "a3": slots.take(1),
    }


def kernel(sizes, *refs):
    nz, ny, nx, rows, chan, depth, taps = sizes
    cv_h, cg_h, co_h, taps_h, gain_h, shift_h, w_h, og_h, gv_v, gg_v, taps_o, gain_o, shift_o, proj_v = refs[:14]
    (co_v, og_v, ogt_v, w_v, cv_v, cg_v, taps_v, gain_v, shift_v, st_s, st_r, s2_s, s2_r, iv_v, sg_v, gt_v, nm_v, ds_v,
     act_v, ag_v, hg_v, gh_s, gh_r, hh_s, hh_r, pxy, pz, fxy, rxy, rzr, rzl, sxy, rxy2, txy, rxy3,
     sz, rz2, tz, rz3, stage, sa, ra, fa, rza, fin, ag_a, in_sem, ssem, rsem) = refs[14:]
    blocks = chan // LANE
    total = 2 * chan
    reach = taps - 1
    plane = ny * nx
    per = stage.shape[0] // plane
    px, fx, rx, sx, rx2, tx, rx3 = (a.at[0] for a in (pxy, fxy, rxy, sxy, rxy2, txy, rxy3))
    py, fy, ry, sy, ry2, ty, ry3 = (a.at[1] for a in (pxy, fxy, rxy, sxy, rxy2, txy, rxy3))
    _, at = layout(nz, ny, nx)
    z, y, x, core = (lax.axis_index(a) for a in ("z", "y", "x", "tp"))
    place = y * nx + x
    line = z * plane + place
    count = nz * plane

    def where(index):
        return {"z": lax.div(index, plane), "y": lax.rem(lax.div(index, nx), ny), "x": lax.rem(index, nx)}

    after = where(lax.rem(line + 1, count))
    before = where(lax.rem(line + count - 1, count))
    other = {"tp": 1 - core}

    def along(axis, size, me, step):
        return {axis: lax.rem(me + step + size, size)}

    def in_plane(step):
        p = lax.rem(place + step, plane)
        return {"y": lax.div(p, nx), "x": lax.rem(p, nx)}

    def remote(src, dst, slot, target):
        return pltpu.make_async_remote_copy(
            src_ref=src, dst_ref=dst, send_sem=ssem.at[slot], recv_sem=rsem.at[slot],
            device_id=target, device_id_type=MESH)

    first_load = pltpu.make_async_copy(co_h, co_v, in_sem.at[0])
    first_load.start()

    barrier = pltpu.get_barrier_semaphore()
    peers = [along("z", nz, z, o) for o in sorted(range(1, nz), key=lambda o: -min(o, nz - o))]
    peers += [in_plane(o) for o in range(plane - 1, 0, -1)]
    peers += [after, before, other]
    for peer in peers:
        pl.semaphore_signal(barrier, inc=1, device_id=peer, device_id_type=MESH)

    loads = {}
    for slot, (name, src, dst) in enumerate((
            ("co", co_h, co_v), ("gain", gain_h, gain_v), ("shift", shift_h, shift_v), ("cg", cg_h, cg_v),
            ("cv", cv_h, cv_v), ("og", og_h, og_v), ("w", w_h, w_v), ("taps", taps_h, taps_v))):
        loads[name] = pltpu.make_async_copy(src, dst, in_sem.at[slot])
        if slot > 0:
            loads[name].start()

    def lanes(b):
        return slice(b * LANE, (b + 1) * LANE)

    loads["co"].wait()

    wide = rows // 2

    def means(i, carry):
        for u in range(wide // 64):
            r = pl.ds(pl.multiple_of(i * wide + u * 64, 64), 64)
            m = jnp.sum(co_v[r, :].astype(F32), axis=1, keepdims=True) * (1.0 / chan)
            st_s[0, r, :] = jnp.broadcast_to(m, (64, LANE))
        return carry

    lax.fori_loop(0, 2, means, 0)

    def spreads(i, carry):
        for u in range(wide // 64):
            r = pl.ds(pl.multiple_of(i * wide + u * 64, 64), 64)
            m = st_s[0, r, :]
            q = jnp.zeros((64, LANE), F32)
            for b in range(blocks):
                d = co_v[r, lanes(b)].astype(F32) - m
                q = q + d * d
            st_s[1, r, :] = jnp.broadcast_to(jnp.sum(q, axis=1, keepdims=True), (64, LANE))
        return carry

    lax.fori_loop(0, 2, spreads, 0)

    pl.semaphore_wait(barrier, len(peers))
    stat_copy = remote(st_s, st_r, at["stat"], other)
    stat_copy.start()
    loads["cg"].wait()
    loads["cv"].wait()

    def gates(i, carry):
        r = pl.ds(pl.multiple_of(i * TILE, TILE), TILE)
        up = pl.ds(pl.multiple_of(i * TILE + HALO, TILE), TILE)
        for b in range(blocks):
            s = 0.5 * jnp.tanh(0.5 * cg_v[r, lanes(b)].astype(F32)) + 0.5
            sg_v[r, lanes(b)] = s
            gt_v[b, up, :] = (cv_v[r, lanes(b)].astype(F32) * s).astype(BF16).astype(F32)
        return carry

    lax.fori_loop(0, rows // TILE, gates, 0)
    for b in range(blocks):
        gh_s[:, lanes(b)] = gt_v[b, rows:rows + HALO, :].astype(BF16)

    gated_copy = remote(gh_s, gh_r, at["gated"], after)

    @pl.when(line < count - 1)
    def _():
        gated_copy.start()


    loads["og"].wait()

    span = plane * 16

    def far(k):
        away = nz // 2 - lax.div(k + 1, 2)
        return lax.rem(z + (2 * lax.rem(k, 2) - 1) * away + nz, nz)

    def turn(k, carry):
        cols = pl.ds(pl.multiple_of(far(k) * span, span), span)
        ogt_v[pl.ds(pl.multiple_of(k * span, span), span), :] = og_v[:, cols].T
        return carry

    lax.fori_loop(0, nz, turn, 0)
    loads["w"].wait()
    ag_v[0:FIRST, :] = jnp.dot(og_v[0:FIRST, :], w_v[...], preferred_element_type=F32)
    loads["gain"].wait()
    loads["shift"].wait()
    stat_copy.wait_recv()

    def norm(i, carry):
        r = pl.ds(pl.multiple_of(i * TILE, TILE), TILE)
        m1, m2 = st_s[0, r, :], st_r[0, r, :]
        gap = m1 - m2
        mean = 0.5 * (m1 + m2)
        inv = lax.rsqrt((st_s[1, r, :] + st_r[1, r, :] + gap * gap * (chan / 2)) * (1.0 / total) + EPS)
        iv_v[r, :] = inv
        for b in range(blocks):
            n = (co_v[r, lanes(b)].astype(F32) - mean) * inv
            s = n * gain_v[lanes(b)].reshape(1, LANE) + shift_v[lanes(b)].reshape(1, LANE)
            sig = 0.5 * jnp.tanh(0.5 * s) + 0.5
            a = s * sig
            act_v[r, lanes(b)] = a.astype(BF16)
            nm_v[r, lanes(b)] = n
            ds_v[r, lanes(b)] = sig + a * (1.0 - sig)
        return carry

    lax.fori_loop(0, rows // TILE, norm, 0)

    third = chan // 3
    half = ny // 2
    stretches = ((0, nz // 2), (nz // 2, nz))
    upper, lower = pl.ds(0, half), pl.ds(half, half)

    def ring(step, leads, src_z, direction):
        buf = rzr if direction > 0 else rzl
        part = upper if leads == (direction > 0) else lower
        slot = at["leads" if leads else "trails"] + step
        return remote(pz.at[src_z, part], buf.at[step, part], slot, along("z", nz, z, direction))

    rings = {"x": (px, fx, rx, x), "y": (py, fy, ry, y)}

    def hop(axis, stretch, kind, direction, lines):
        wide, far_got, got, me = rings[axis]
        d = 0 if direction > 0 else 1
        mine, rest = (upper, lower) if direction > 0 else (lower, upper)
        slot = at["far" if kind == FAR else "near"] + stretch
        peer = along(axis, 4, me, direction)
        if kind == FAR:
            return remote(wide.at[lax.rem(me + 2, 4), lines, mine], far_got.at[d, lines], slot, peer)
        part = rest if kind == NEAR else mine
        return remote(wide.at[peer[axis], lines, part], got.at[d, lines, part], slot, peer)

    def relay(stretch):
        lo, hi = stretches[stretch]
        part = fxy.at[:, :, pl.ds(0, hi - lo)]
        remote(part, part, at["far"] + stretch, other).wait_recv()
        for axis in ("x", "y"):
            wide, far_got, _, me = rings[axis]
            for direction in (1, -1):
                d, first = (0, 0) if direction > 0 else (1, half)
                dest = lax.rem(me + direction + 4, 4)

                def step(k, carry):
                    for w in range(half):
                        v = wide[dest, k, first + w].astype(F32) + far_got[d, k, w].astype(F32)
                        wide[dest, k, first + w] = v.astype(BF16)
                    return carry

                lax.fori_loop(lo, hi, step, 0)
                hop(axis, stretch, SUM, direction, pl.ds(lo, hi - lo)).start()

    def ring_wait(step, leads):
        return remote(pz.at[0], pz.at[0], at["leads" if leads else "trails"] + step, other)

    def project(stretch):
        def step(i, carry):
            lines = pl.ds(pl.multiple_of(i * 2 * span, span), 2 * span)
            both = jnp.dot(ogt_v[lines, :], act_v[...], preferred_element_type=F32)
            for u in range(2):
                k = 2 * i + u
                zz = far(k)
                block = both[u * span:(u + 1) * span].astype(BF16)
                for yy in range(ny):
                    for xx in range(nx):
                        part = slice((yy * nx + xx) * 16, (yy * nx + xx) * 16 + 16)
                        px[xx, k, yy] = block[part, 0:third]
                        py[yy, k, xx] = block[part, third:2 * third]
                        pz[zz, yy, xx] = block[part, 2 * third:]
            if stretch == 0:
                @pl.when(i == 0)
                def _():
                    for direction in (1, -1):
                        ring(0, True, far(0), direction).start()
                    ring(1, False, far(1), 1).start()

                @pl.when(i == 1)
                def _():
                    ring(1, False, far(2), -1).start()

            return carry

        lo, hi = stretches[stretch]
        lax.fori_loop(lo // 2, hi // 2, step, 0)
        for kind in (FAR, NEAR):
            for axis in ("x", "y"):
                for direction in (1, -1):
                    hop(axis, stretch, kind, direction, pl.ds(lo, hi - lo)).start()

    def z_step(step, leads):
        ring_wait(step - 1, leads).wait_recv()
        for direction in (1, -1):
            dest = lax.rem(z + direction * (nz // 2 - step) + nz, nz)
            buf = rzr if direction > 0 else rzl
            for yy in (range(half) if leads == (direction > 0) else range(half, ny)):
                pz[dest, yy] = (pz[dest, yy].astype(F32) + buf[step - 1, yy].astype(F32)).astype(BF16)
            ring(step, leads, dest, direction).start()

    project(0)

    ag_v[FIRST:, :] = jnp.dot(og_v[FIRST:, :], w_v[...], preferred_element_type=F32)

    def grads(i, carry):
        r = pl.ds(pl.multiple_of(i * TILE, TILE), TILE)
        carry = list(carry)
        row_sum = jnp.zeros((TILE, LANE), F32)
        row_dot = jnp.zeros((TILE, LANE), F32)
        for b in range(blocks):
            g = ag_v[r, lanes(b)] * ds_v[r, lanes(b)]
            n = nm_v[r, lanes(b)]
            gn = g * n
            carry[b] = carry[b] + jnp.sum(gn.reshape(TILE // 8, 8, LANE), axis=0)
            carry[blocks + b] = carry[blocks + b] + jnp.sum(g.reshape(TILE // 8, 8, LANE), axis=0)
            gain = gain_v[lanes(b)].reshape(1, LANE)
            s = g * gain
            ag_v[r, lanes(b)] = s
            row_sum = row_sum + s
            row_dot = row_dot + gn * gain
        s2_s[0, r, :] = row_sum
        s2_s[1, r, :] = row_dot
        return tuple(carry)

    def channel_sums(i):
        for u in range(wide // 64):
            r = pl.ds(i * wide + u * 64, 64)
            for w in range(2):
                v = jnp.sum(s2_s[w, r, :], axis=1, keepdims=True)
                s2_s[w, r, :] = jnp.broadcast_to(v, (64, LANE))

    partial = tuple(jnp.zeros((8, LANE), F32) for _ in range(2 * blocks))
    for i in range(2):
        partial = lax.fori_loop(i * wide // TILE, (i + 1) * wide // TILE, grads, partial)
        channel_sums(i)
        part = pl.ds(i * wide, wide)
        remote(s2_s.at[:, part], s2_r.at[:, part], at["sums"], other).start()
    sums_copy = remote(s2_s, s2_r, at["sums"], other)

    project(1)
    relay(0)
    z_step(1, True)

    @pl.when(line > 0)
    def _():
        gated_copy.wait_recv()

    for b in range(blocks):
        head = gh_r[:, lanes(b)].astype(F32)
        gt_v[b, 0:HALO, :] = jnp.where(line == 0, 0.0, head)

    sums_copy.wait_recv()

    def height(i, carry):
        r = pl.ds(pl.multiple_of(i * TILE, TILE), TILE)
        sums = (s2_s[0, r, :] + s2_r[0, r, :]) * (1.0 / total)
        dots = (s2_s[1, r, :] + s2_r[1, r, :]) * (1.0 / total)
        inv = iv_v[r, :]
        for b in range(blocks):
            hg_v[b, r, :] = inv * (ag_v[r, lanes(b)] - sums - nm_v[r, lanes(b)] * dots)
        return carry

    lax.fori_loop(0, rows // TILE, height, 0)
    for b in range(blocks):
        hh_s[:, lanes(b)] = hg_v[b, 0:HALO, :].astype(BF16)
    height_copy = remote(hh_s, hh_r, at["height"], before)

    @pl.when(line > 0)
    def _():
        height_copy.start()


    def gather(stretch, wide, me, got, out, got2, axis, size, own_me):
        lo, hi = stretches[stretch]

        def step(k, carry):
            v = (wide[me, k].astype(F32) + got[0, k].astype(F32) + got[1, k].astype(F32)).astype(BF16)
            for w in range(size):
                out[w, k] = v[w]
            return carry

        lax.fori_loop(lo, hi, step, 0)
        some = pl.ds(lo, hi - lo)
        for o in range(1, size):
            peer = along(axis, size, own_me, o)
            remote(out.at[peer[axis], some], got2.at[o - 1, some], at["second"] + stretch, peer).start()

    def gather_both(stretch):
        lo, hi = stretches[stretch]
        part = rxy.at[:, :, pl.ds(0, hi - lo)]
        remote(part, part, at["near"] + stretch, other).wait_recv()
        gather(stretch, px, x, rx, sx, rx2, "y", ny, y)
        gather(stretch, py, y, ry, sy, ry2, "x", nx, x)

    used = blocks * (taps + 2)
    stage[used:, :] = jnp.zeros((stage.shape[0] - used, LANE), F32)

    def tap_block(b):
        def step(t, acc):
            base = t * (8 * GROUP)
            h = [hg_v[b, pl.ds(pl.multiple_of(base + 8 * u, 8), 8), :] for u in range(GROUP)]
            acc = list(acc)
            for k in range(taps + 8 * (GROUP - 1)):
                v = gt_v[b, pl.ds(base + (HALO - reach) + k, 8), :]
                for u in range(GROUP):
                    if 0 <= k - 8 * u < taps:
                        acc[k - 8 * u] = acc[k - 8 * u] + h[u] * v
            return tuple(acc)

        acc = lax.fori_loop(
            0, rows // (8 * GROUP), step, tuple(jnp.zeros((8, LANE), F32) for _ in range(taps)))
        acc = list(acc) + [partial[b], partial[blocks + b]]
        for j, a in enumerate(acc):
            row = b * (taps + 2) + j
            stage[row:row + 1, :] = jnp.sum(a, axis=0, keepdims=True)

    for b in range(blocks):
        tap_block(b)
        if b == 1:
            z_step(2, False)
        if b == 4:
            z_step(2, True)
            relay(1)
    for p in range(plane):
        sa[p] = stage[p * per:(p + 1) * per, :].astype(BF16)
    for o in range(1, plane):
        remote(sa.at[lax.rem(place + o, plane)], ra.at[o - 1], at["a1"], in_plane(o)).start()

    def z_done():
        for leads in (False, True):
            ring_wait(nz // 2 - 1, leads).wait_recv()
        for yy in range(ny):
            v = pz[z, yy].astype(F32) + rzr[nz // 2 - 1, yy].astype(F32) + rzl[nz // 2 - 1, yy].astype(F32)
            v = v.astype(BF16)
            for xx in range(nx):
                sz[xx, yy] = v[xx]
        for o in range(1, nx):
            peer = along("x", nx, x, o)
            remote(sz.at[peer["x"]], rz2.at[o - 1], at["z2"], peer).start()

    def small_plane():
        remote(ra, ra, at["a1"], other).wait_recv()
        v = stage[pl.ds(pl.multiple_of(place * per, 8), per), :]
        for o in range(plane - 1):
            v = v + ra[o].astype(F32)
        fa[...] = v.astype(BF16)
        rza[z] = v.astype(BF16)
        for o in range(1, nz):
            remote(fa, rza.at[z], at["a2"], along("z", nz, z, o)).start()

    def xy_third(stretch, own, me, got, out, last, size):
        lo, hi = stretches[stretch]
        def step(k, carry):
            zz = far(k)
            v = own[me, k].astype(F32)
            for o in range(size - 1):
                v = v + got[o, k].astype(F32)
            out[k] = v.astype(BF16)

            @pl.when(k < nz - 1)
            def _():
                o = lax.rem(zz - z + nz, nz)
                remote(out.at[k], last.at[o - 1], at["last"], {"z": zz}).start()

            return carry

        lax.fori_loop(lo, hi, step, 0)

    def third_both(stretch):
        lo, hi = stretches[stretch]
        part = rxy2.at[:, :, pl.ds(0, hi - lo)]
        remote(part, part, at["second"] + stretch, other).wait_recv()
        xy_third(stretch, sx, y, rx2, tx, rx3, ny)
        xy_third(stretch, sy, x, ry2, ty, ry3, nx)

    def z_third():
        remote(rz2, rz2, at["z2"], other).wait_recv()
        v = sz[x].astype(F32)
        for o in range(nx - 1):
            v = v + rz2[o].astype(F32)
        tz[...] = v.astype(BF16)
        for o in range(1, ny):
            peer = along("y", ny, y, o)
            remote(tz.at[peer["y"]], rz3.at[o - 1], at["z3"], peer).start()

    def small_line():
        rest = rza.at[pl.ds(0, nz - 1)]
        remote(rest, rest, at["a2"], other).wait_recv()
        v = rza[0].astype(F32)
        for zz in range(1, nz):
            v = v + rza[zz].astype(F32)
        fin[...] = v.astype(BF16)
        ag_a[place] = v.astype(BF16)
        for o in range(1, plane):
            remote(fin, ag_a.at[place], at["a3"], in_plane(o)).start()

    z_step(3, False)
    gather_both(0)

    @pl.when(line < count - 1)
    def _():
        height_copy.wait_recv()

    for b in range(blocks):
        tail = hh_r[:, lanes(b)].astype(F32)
        hg_v[b, rows:rows + HALO, :] = jnp.where(line == count - 1, 0.0, tail)

    loads["taps"].wait()

    def gated_block(b):
        lines = taps_v[:, lanes(b)].astype(F32)
        spread = [jnp.broadcast_to(lines[j:j + 1, :], (8, LANE)) for j in range(taps)]

        def step(t, carry):
            base = t * (8 * GROUP)
            acc = [None] * GROUP
            for k in range(taps + 8 * (GROUP - 1)):
                v = hg_v[b, pl.ds(base + k, 8), :]
                for u in range(GROUP):
                    j = reach + 8 * u - k
                    if 0 <= j < taps:
                        term = spread[j] * v
                        acc[u] = term if acc[u] is None else acc[u] + term
            for u in range(0, GROUP, 2):
                r = pl.ds(pl.multiple_of(base + 8 * u, 16), 16)
                g = jnp.concatenate(acc[u:u + 2], axis=0)
                s = sg_v[r, lanes(b)]
                gs = g * s
                gv_v[r, lanes(b)] = gs.astype(BF16)
                gg_v[r, lanes(b)] = (gs * cv_v[r, lanes(b)].astype(F32) * (1.0 - s)).astype(BF16)
            return carry

        lax.fori_loop(0, rows // (8 * GROUP), step, 0)

    for b in range(blocks):
        gated_block(b)
        if b == 1:
            z_step(3, True)
            gather_both(1)
        if b == 2:
            small_plane()
        if b == 3:
            z_done()
            third_both(0)
        if b == 4:
            third_both(1)
        if b == 5:
            small_line()
            z_third()

    remote(rxy3, rxy3, at["last"], other).wait_recv()
    for buf, own, last in ((0, tx, rx3), (1, ty, ry3)):
        v = own[nz - 1].astype(F32)
        for o in range(nz - 1):
            v = v + last[o].astype(F32)
        proj_v[:, buf * third:(buf + 1) * third] = v
    remote(rz3, rz3, at["z3"], other).wait_recv()
    v = tz[y].astype(F32)
    for o in range(ny - 1):
        v = v + rz3[o].astype(F32)
    proj_v[:, 2 * third:] = v

    rest = ag_a.at[pl.ds(0, plane - 1)]
    remote(rest, rest, at["a3"], other).wait_recv()
    for p in range(plane):
        stage[p * per:(p + 1) * per, :] = ag_a[p].astype(F32)
    for b in range(blocks):
        for j in range(taps + 2):
            row = b * (taps + 2) + j
            v = stage[row:row + 1, :]
            if j < taps:
                taps_o[j:j + 1, lanes(b)] = v
            else:
                (gain_o if j == taps else shift_o)[lanes(b)] = v.reshape(LANE)

    stat_copy.wait_send()

    @pl.when(line < count - 1)
    def _():
        gated_copy.wait_send()

    sums_copy.wait_send()

    @pl.when(line > 0)
    def _():
        height_copy.wait_send()

    for stretch, (lo, hi) in enumerate(stretches):
        some = pl.ds(0, hi - lo)
        for name, buf in (("far", fxy), ("near", rxy), ("second", rxy2)):
            part = buf.at[:, :, some]
            remote(part, part, at[name] + stretch, other).wait_send()
    for step in range(nz // 2):
        ring_wait(step, True).wait_send()
        if step > 0:
            ring_wait(step, False).wait_send()
    for name, part in (("last", rxy3), ("z2", rz2), ("z3", rz3), ("a1", ra), ("a2", rza.at[pl.ds(0, nz - 1)]), ("a3", rest)):
        remote(part, part, at[name], other).wait_send()


def local(conv_value, conv_gate, conv_out, conv_taps, norm_gain, norm_shift, proj_weight, out_grad):
    nz, ny, nx = (lax.axis_size(a) for a in SP)
    rows, chan = conv_value.shape
    depth = out_grad.shape[1]
    taps = conv_taps.shape[0]
    blocks = chan // LANE
    third = chan // 3
    plane = ny * nx
    slots, _ = layout(nz, ny, nx)
    vm = pltpu.VMEM
    per = -(-(blocks * (taps + 2)) // (16 * plane)) * 16
    scratch = [
        vm((rows, chan), BF16), vm((rows, depth), BF16), vm((depth, rows), BF16), vm((depth, chan), BF16), vm((rows, chan), BF16),
        vm((rows, chan), BF16), vm((taps, chan), BF16), vm((chan,), F32), vm((chan,), F32),
        vm((2, rows, LANE), F32), vm((2, rows, LANE), F32), vm((2, rows, LANE), F32), vm((2, rows, LANE), F32),
        vm((rows, LANE), F32), vm((rows, chan), F32), vm((blocks, rows + HALO, LANE), F32), vm((rows, chan), F32),
        vm((rows, chan), F32), vm((rows, chan), BF16), vm((rows, chan), F32), vm((blocks, rows + HALO, LANE), F32),
        vm((HALO, chan), BF16), vm((HALO, chan), BF16), vm((HALO, chan), BF16), vm((HALO, chan), BF16),
        vm((2, 4, nz, 4, 16, third), BF16), vm((nz, 4, 4, 16, third), BF16),
        vm((2, 2, nz, 2, 16, third), BF16), vm((2, 2, nz, 4, 16, third), BF16),
        vm((nz // 2, 4, 4, 16, third), BF16), vm((nz // 2, 4, 4, 16, third), BF16),
        vm((2, 4, nz, 16, third), BF16), vm((2, 3, nz, 16, third), BF16),
        vm((2, nz, 16, third), BF16), vm((2, nz - 1, 16, third), BF16),
        vm((nx, ny, 16, third), BF16), vm((nx - 1, ny, 16, third), BF16),
        vm((ny, 16, third), BF16), vm((ny - 1, 16, third), BF16),
        vm((plane * per, LANE), F32), vm((plane, per, LANE), BF16), vm((plane - 1, per, LANE), BF16), vm((per, LANE), BF16),
        vm((nz, per, LANE), BF16), vm((per, LANE), BF16), vm((plane, per, LANE), BF16),
        pltpu.SemaphoreType.DMA((8,)),
        pltpu.SemaphoreType.DMA((slots.used,)), pltpu.SemaphoreType.DMA((slots.used,)),
    ]
    anywhere = pl.BlockSpec(memory_space=pl.ANY)
    shapes = (
        ((rows, chan), BF16), ((rows, chan), BF16), ((taps, chan), F32), ((chan,), F32), ((chan,), F32), ((16, chan), F32),
    )
    held = pl.BlockSpec(memory_space=pltpu.VMEM)
    results = pl.pallas_call(
        functools.partial(kernel, (nz, ny, nx, rows, chan, depth, taps)),
        out_shape=tuple(pltpu.VMEM(*s) for s in shapes),
        in_specs=[anywhere] * 8,
        out_specs=(held,) * 6,
        scratch_shapes=scratch,
        compiler_params=pltpu.CompilerParams(
            collective_id=0, has_side_effects=True, vmem_limit_bytes=36 * 1024 * 1024),
        name="module_backward",
    )(*(pltpu.with_memory_space_constraint(a, pltpu.HBM) for a in (
        conv_value, conv_gate, conv_out, conv_taps, norm_gain, norm_shift, proj_weight, out_grad)))
    return pl.pallas_call(
        write_out,
        out_shape=tuple(jax.ShapeDtypeStruct(*s) for s in shapes),
        in_specs=[held] * 6,
        out_specs=(anywhere,) * 6,
        scratch_shapes=[pltpu.SemaphoreType.DMA((6,))],
        name="write_out",
    )(*(pltpu.with_memory_space_constraint(a, pltpu.VMEM) for a in results))


def write_out(*refs):
    sem = refs[12]
    copies = [pltpu.make_async_copy(refs[i], refs[6 + i], sem.at[i]) for i in range(6)]
    for c in copies:
        c.start()
    for c in copies:
        c.wait()


def solution(mesh):
    split = Mesh(mesh.devices.reshape(8, 4, 4, mesh.shape["tp"]), (*SP, "tp"))
    placed = (
        P(SP, "tp"), P(SP, "tp"), P(SP, "tp"), P(None, "tp"), P("tp"), P("tp"), P(None, "tp"), P(SP, None),
    )
    return jax.shard_map(
        local,
        mesh=split,
        in_specs=placed,
        out_specs=(P(SP, "tp"), P(SP, "tp"), P(None, "tp"), P("tp"), P("tp"), P(SP, "tp")),
        check_vma=False,
    )
```

```python
import functools

import jax
import jax.numpy as jnp
from jax import lax
from jax.experimental import pallas as pl
from jax.experimental.pallas import tpu as pltpu
from jax.sharding import Mesh
from jax.sharding import PartitionSpec as P

MESH = pl.DeviceIdType.MESH
F32 = jnp.float32
BF16 = jnp.bfloat16
SP = ("z", "y", "x")
EPS = 1e-05
HALO = 32
LANE = 128
TILE = 32
GROUP = 8
FIRST = 128
FAR, NEAR, SUM = range(3)


class Slots:
    def __init__(self):
        self.used = 0

    def take(self, count):
        first = self.used
        self.used += count
        return first


def layout(nz, ny, nx):
    slots = Slots()
    plane = ny * nx
    return slots, {
        "stat": slots.take(1),
        "sums": slots.take(1),
        "gated": slots.take(1),
        "height": slots.take(1),
        "far": slots.take(2),
        "near": slots.take(2),
        "second": slots.take(2),
        "last": slots.take(1),
        "leads": slots.take(nz // 2),
        "trails": slots.take(nz // 2),
        "z2": slots.take(1),
        "z3": slots.take(1),
        "a1": slots.take(1),
        "a2": slots.take(1),
        "a3": slots.take(1),
    }


def kernel(sizes, *refs):
    nz, ny, nx, rows, chan, depth, taps = sizes
    cv_h, cg_h, co_h, taps_h, gain_h, shift_h, w_h, og_h, gv_v, gg_v, taps_o, gain_o, shift_o, proj_v = refs[:14]
    (co_v, og_v, ogt_v, w_v, cv_v, cg_v, taps_v, gain_v, shift_v, st_s, st_r, s2_s, s2_r, iv_v, sg_v, gt_v, nm_v, ds_v,
     act_v, ag_v, hg_v, gh_s, gh_r, hh_s, hh_r, pxy, pz, fxy, rxy, rzr, rzl, sxy, rxy2, txy, rxy3,
     sz, rz2, tz, rz3, stage, sa, ra, fa, rza, fin, ag_a, in_sem, ssem, rsem) = refs[14:]
    blocks = chan // LANE
    total = 2 * chan
    reach = taps - 1
    plane = ny * nx
    per = stage.shape[0] // plane
    px, fx, rx, sx, rx2, tx, rx3 = (a.at[0] for a in (pxy, fxy, rxy, sxy, rxy2, txy, rxy3))
    py, fy, ry, sy, ry2, ty, ry3 = (a.at[1] for a in (pxy, fxy, rxy, sxy, rxy2, txy, rxy3))
    _, at = layout(nz, ny, nx)
    z, y, x, core = (lax.axis_index(a) for a in ("z", "y", "x", "tp"))
    place = y * nx + x
    line = z * plane + place
    count = nz * plane

    def where(index):
        return {"z": lax.div(index, plane), "y": lax.rem(lax.div(index, nx), ny), "x": lax.rem(index, nx)}

    after = where(lax.rem(line + 1, count))
    before = where(lax.rem(line + count - 1, count))
    other = {"tp": 1 - core}

    def along(axis, size, me, step):
        return {axis: lax.rem(me + step + size, size)}

    def in_plane(step):
        p = lax.rem(place + step, plane)
        return {"y": lax.div(p, nx), "x": lax.rem(p, nx)}

    def remote(src, dst, slot, target):
        return pltpu.make_async_remote_copy(
            src_ref=src, dst_ref=dst, send_sem=ssem.at[slot], recv_sem=rsem.at[slot],
            device_id=target, device_id_type=MESH)

    first_load = pltpu.make_async_copy(co_h, co_v, in_sem.at[0])
    first_load.start()

    barrier = pltpu.get_barrier_semaphore()
    peers = [along("z", nz, z, o) for o in sorted(range(1, nz), key=lambda o: -min(o, nz - o))]
    peers += [in_plane(o) for o in range(plane - 1, 0, -1)]
    peers += [after, before, other]
    for peer in peers:
        pl.semaphore_signal(barrier, inc=1, device_id=peer, device_id_type=MESH)

    loads = {}
    for slot, (name, src, dst) in enumerate((
            ("co", co_h, co_v), ("gain", gain_h, gain_v), ("shift", shift_h, shift_v), ("cg", cg_h, cg_v),
            ("cv", cv_h, cv_v), ("og", og_h, og_v), ("w", w_h, w_v), ("taps", taps_h, taps_v))):
        loads[name] = pltpu.make_async_copy(src, dst, in_sem.at[slot])
        if slot > 0:
            loads[name].start()

    def lanes(b):
        return slice(b * LANE, (b + 1) * LANE)

    loads["co"].wait()

    wide = rows // 2

    def means(i, carry):
        for u in range(wide // 64):
            r = pl.ds(pl.multiple_of(i * wide + u * 64, 64), 64)
            m = jnp.sum(co_v[r, :].astype(F32), axis=1, keepdims=True) * (1.0 / chan)
            st_s[0, r, :] = jnp.broadcast_to(m, (64, LANE))
        return carry

    lax.fori_loop(0, 2, means, 0)

    def spreads(i, carry):
        for u in range(wide // 64):
            r = pl.ds(pl.multiple_of(i * wide + u * 64, 64), 64)
            m = st_s[0, r, :]
            q = jnp.zeros((64, LANE), F32)
            for b in range(blocks):
                d = co_v[r, lanes(b)].astype(F32) - m
                q = q + d * d
            st_s[1, r, :] = jnp.broadcast_to(jnp.sum(q, axis=1, keepdims=True), (64, LANE))
        return carry

    lax.fori_loop(0, 2, spreads, 0)

    pl.semaphore_wait(barrier, len(peers))
    stat_copy = remote(st_s, st_r, at["stat"], other)
    stat_copy.start()
    loads["cg"].wait()
    loads["cv"].wait()

    def gates(i, carry):
        r = pl.ds(pl.multiple_of(i * TILE, TILE), TILE)
        up = pl.ds(pl.multiple_of(i * TILE + HALO, TILE), TILE)
        for b in range(blocks):
            s = 0.5 * jnp.tanh(0.5 * cg_v[r, lanes(b)].astype(F32)) + 0.5
            sg_v[r, lanes(b)] = s
            gt_v[b, up, :] = (cv_v[r, lanes(b)].astype(F32) * s).astype(BF16).astype(F32)
        return carry

    lax.fori_loop(0, rows // TILE, gates, 0)
    for b in range(blocks):
        gh_s[:, lanes(b)] = gt_v[b, rows:rows + HALO, :].astype(BF16)

    gated_copy = remote(gh_s, gh_r, at["gated"], after)

    @pl.when(line < count - 1)
    def _():
        gated_copy.start()


    loads["og"].wait()

    span = plane * 16

    def far(k):
        away = nz // 2 - lax.div(k + 1, 2)
        return lax.rem(z + (2 * lax.rem(k, 2) - 1) * away + nz, nz)

    def turn(k, carry):
        cols = pl.ds(pl.multiple_of(far(k) * span, span), span)
        ogt_v[pl.ds(pl.multiple_of(k * span, span), span), :] = og_v[:, cols].T
        return carry

    lax.fori_loop(0, nz, turn, 0)
    loads["w"].wait()
    ag_v[0:FIRST, :] = jnp.dot(og_v[0:FIRST, :], w_v[...], preferred_element_type=F32)
    loads["gain"].wait()
    loads["shift"].wait()
    stat_copy.wait_recv()

    def norm(i, carry):
        r = pl.ds(pl.multiple_of(i * TILE, TILE), TILE)
        m1, m2 = st_s[0, r, :], st_r[0, r, :]
        gap = m1 - m2
        mean = 0.5 * (m1 + m2)
        inv = lax.rsqrt((st_s[1, r, :] + st_r[1, r, :] + gap * gap * (chan / 2)) * (1.0 / total) + EPS)
        iv_v[r, :] = inv
        for b in range(blocks):
            n = (co_v[r, lanes(b)].astype(F32) - mean) * inv
            s = n * gain_v[lanes(b)].reshape(1, LANE) + shift_v[lanes(b)].reshape(1, LANE)
            sig = 0.5 * jnp.tanh(0.5 * s) + 0.5
            a = s * sig
            act_v[r, lanes(b)] = a.astype(BF16)
            nm_v[r, lanes(b)] = n
            ds_v[r, lanes(b)] = sig + a * (1.0 - sig)
        return carry

    lax.fori_loop(0, rows // TILE, norm, 0)

    third = chan // 3
    half = ny // 2
    stretches = ((0, nz // 2), (nz // 2, nz))
    upper, lower = pl.ds(0, half), pl.ds(half, half)

    def ring(step, leads, src_z, direction):
        buf = rzr if direction > 0 else rzl
        part = upper if leads == (direction > 0) else lower
        slot = at["leads" if leads else "trails"] + step
        return remote(pz.at[src_z, part], buf.at[step, part], slot, along("z", nz, z, direction))

    rings = {"x": (px, fx, rx, x), "y": (py, fy, ry, y)}

    def hop(axis, stretch, kind, direction, lines):
        wide, far_got, got, me = rings[axis]
        d = 0 if direction > 0 else 1
        mine, rest = (upper, lower) if direction > 0 else (lower, upper)
        slot = at["far" if kind == FAR else "near"] + stretch
        peer = along(axis, 4, me, direction)
        if kind == FAR:
            return remote(wide.at[lax.rem(me + 2, 4), lines, mine], far_got.at[d, lines], slot, peer)
        part = rest if kind == NEAR else mine
        return remote(wide.at[peer[axis], lines, part], got.at[d, lines, part], slot, peer)

    def relay(stretch):
        lo, hi = stretches[stretch]
        part = fxy.at[:, :, pl.ds(0, hi - lo)]
        remote(part, part, at["far"] + stretch, other).wait_recv()
        for axis in ("x", "y"):
            wide, far_got, _, me = rings[axis]
            for direction in (1, -1):
                d, first = (0, 0) if direction > 0 else (1, half)
                dest = lax.rem(me + direction + 4, 4)

                def step(k, carry):
                    for w in range(half):
                        v = wide[dest, k, first + w].astype(F32) + far_got[d, k, w].astype(F32)
                        wide[dest, k, first + w] = v.astype(BF16)
                    return carry

                lax.fori_loop(lo, hi, step, 0)
                hop(axis, stretch, SUM, direction, pl.ds(lo, hi - lo)).start()

    def ring_wait(step, leads):
        return remote(pz.at[0], pz.at[0], at["leads" if leads else "trails"] + step, other)

    def send(stretch, kind):
        lo, hi = stretches[stretch]
        for axis in ("x", "y"):
            for direction in (1, -1):
                hop(axis, stretch, kind, direction, pl.ds(lo, hi - lo)).start()

    def project(stretch):
        def step(i, carry):
            lines = pl.ds(pl.multiple_of(i * 2 * span, span), 2 * span)
            both = jnp.dot(ogt_v[lines, :], act_v[...], preferred_element_type=F32)
            for u in range(2):
                k = 2 * i + u
                zz = far(k)
                block = both[u * span:(u + 1) * span].astype(BF16)
                for yy in range(ny):
                    for xx in range(nx):
                        part = slice((yy * nx + xx) * 16, (yy * nx + xx) * 16 + 16)
                        px[xx, k, yy] = block[part, 0:third]
                        py[yy, k, xx] = block[part, third:2 * third]
                        pz[zz, yy, xx] = block[part, 2 * third:]
            if stretch == 0:
                @pl.when(i == 0)
                def _():
                    for direction in (1, -1):
                        ring(0, True, far(0), direction).start()
                    ring(1, False, far(1), 1).start()

                @pl.when(i == 1)
                def _():
                    ring(1, False, far(2), -1).start()

            return carry

        lo, hi = stretches[stretch]
        lax.fori_loop(lo // 2, hi // 2, step, 0)
        send(stretch, FAR)

    def z_step(step, leads):
        ring_wait(step - 1, leads).wait_recv()
        for direction in (1, -1):
            dest = lax.rem(z + direction * (nz // 2 - step) + nz, nz)
            buf = rzr if direction > 0 else rzl
            for yy in (range(half) if leads == (direction > 0) else range(half, ny)):
                pz[dest, yy] = (pz[dest, yy].astype(F32) + buf[step - 1, yy].astype(F32)).astype(BF16)
            ring(step, leads, dest, direction).start()

    project(0)
    send(0, NEAR)

    ag_v[FIRST:, :] = jnp.dot(og_v[FIRST:, :], w_v[...], preferred_element_type=F32)

    def grads(i, carry):
        r = pl.ds(pl.multiple_of(i * TILE, TILE), TILE)
        carry = list(carry)
        row_sum = jnp.zeros((TILE, LANE), F32)
        row_dot = jnp.zeros((TILE, LANE), F32)
        for b in range(blocks):
            g = ag_v[r, lanes(b)] * ds_v[r, lanes(b)]
            n = nm_v[r, lanes(b)]
            gn = g * n
            carry[b] = carry[b] + jnp.sum(gn.reshape(TILE // 8, 8, LANE), axis=0)
            carry[blocks + b] = carry[blocks + b] + jnp.sum(g.reshape(TILE // 8, 8, LANE), axis=0)
            gain = gain_v[lanes(b)].reshape(1, LANE)
            s = g * gain
            ag_v[r, lanes(b)] = s
            row_sum = row_sum + s
            row_dot = row_dot + gn * gain
        s2_s[0, r, :] = row_sum
        s2_s[1, r, :] = row_dot
        return tuple(carry)

    def channel_sums(i):
        for u in range(wide // 64):
            r = pl.ds(i * wide + u * 64, 64)
            for w in range(2):
                v = jnp.sum(s2_s[w, r, :], axis=1, keepdims=True)
                s2_s[w, r, :] = jnp.broadcast_to(v, (64, LANE))

    partial = tuple(jnp.zeros((8, LANE), F32) for _ in range(2 * blocks))
    for i in range(2):
        partial = lax.fori_loop(i * wide // TILE, (i + 1) * wide // TILE, grads, partial)
        channel_sums(i)
        part = pl.ds(i * wide, wide)
        remote(s2_s.at[:, part], s2_r.at[:, part], at["sums"], other).start()
    sums_copy = remote(s2_s, s2_r, at["sums"], other)

    project(1)
    relay(0)
    send(1, NEAR)
    z_step(1, True)

    @pl.when(line > 0)
    def _():
        gated_copy.wait_recv()

    for b in range(blocks):
        head = gh_r[:, lanes(b)].astype(F32)
        gt_v[b, 0:HALO, :] = jnp.where(line == 0, 0.0, head)

    sums_copy.wait_recv()

    def height(i, carry):
        r = pl.ds(pl.multiple_of(i * TILE, TILE), TILE)
        sums = (s2_s[0, r, :] + s2_r[0, r, :]) * (1.0 / total)
        dots = (s2_s[1, r, :] + s2_r[1, r, :]) * (1.0 / total)
        inv = iv_v[r, :]
        for b in range(blocks):
            hg_v[b, r, :] = inv * (ag_v[r, lanes(b)] - sums - nm_v[r, lanes(b)] * dots)
        return carry

    lax.fori_loop(0, rows // TILE, height, 0)
    for b in range(blocks):
        hh_s[:, lanes(b)] = hg_v[b, 0:HALO, :].astype(BF16)
    height_copy = remote(hh_s, hh_r, at["height"], before)

    @pl.when(line > 0)
    def _():
        height_copy.start()


    def gather(stretch, wide, me, got, out, got2, axis, size, own_me):
        lo, hi = stretches[stretch]

        def step(k, carry):
            v = (wide[me, k].astype(F32) + got[0, k].astype(F32) + got[1, k].astype(F32)).astype(BF16)
            for w in range(size):
                out[w, k] = v[w]
            return carry

        lax.fori_loop(lo, hi, step, 0)
        some = pl.ds(lo, hi - lo)
        for o in range(1, size):
            peer = along(axis, size, own_me, o)
            remote(out.at[peer[axis], some], got2.at[o - 1, some], at["second"] + stretch, peer).start()

    def gather_both(stretch):
        lo, hi = stretches[stretch]
        part = rxy.at[:, :, pl.ds(0, hi - lo)]
        remote(part, part, at["near"] + stretch, other).wait_recv()
        gather(stretch, px, x, rx, sx, rx2, "y", ny, y)
        gather(stretch, py, y, ry, sy, ry2, "x", nx, x)

    used = blocks * (taps + 2)
    stage[used:, :] = jnp.zeros((stage.shape[0] - used, LANE), F32)

    def tap_block(b):
        def step(t, acc):
            base = t * (8 * GROUP)
            h = [hg_v[b, pl.ds(pl.multiple_of(base + 8 * u, 8), 8), :] for u in range(GROUP)]
            acc = list(acc)
            for k in range(taps + 8 * (GROUP - 1)):
                v = gt_v[b, pl.ds(base + (HALO - reach) + k, 8), :]
                for u in range(GROUP):
                    if 0 <= k - 8 * u < taps:
                        acc[k - 8 * u] = acc[k - 8 * u] + h[u] * v
            return tuple(acc)

        acc = lax.fori_loop(
            0, rows // (8 * GROUP), step, tuple(jnp.zeros((8, LANE), F32) for _ in range(taps)))
        acc = list(acc) + [partial[b], partial[blocks + b]]
        for j, a in enumerate(acc):
            row = b * (taps + 2) + j
            stage[row:row + 1, :] = jnp.sum(a, axis=0, keepdims=True)

    for b in range(blocks):
        tap_block(b)
        if b == 1:
            z_step(2, False)
        if b == 4:
            z_step(2, True)
            relay(1)
    for p in range(plane):
        sa[p] = stage[p * per:(p + 1) * per, :].astype(BF16)
    for o in range(1, plane):
        remote(sa.at[lax.rem(place + o, plane)], ra.at[o - 1], at["a1"], in_plane(o)).start()

    def z_done():
        for leads in (False, True):
            ring_wait(nz // 2 - 1, leads).wait_recv()
        for yy in range(ny):
            v = pz[z, yy].astype(F32) + rzr[nz // 2 - 1, yy].astype(F32) + rzl[nz // 2 - 1, yy].astype(F32)
            v = v.astype(BF16)
            for xx in range(nx):
                sz[xx, yy] = v[xx]
        for o in range(1, nx):
            peer = along("x", nx, x, o)
            remote(sz.at[peer["x"]], rz2.at[o - 1], at["z2"], peer).start()

    def small_plane():
        remote(ra, ra, at["a1"], other).wait_recv()
        v = stage[pl.ds(pl.multiple_of(place * per, 8), per), :]
        for o in range(plane - 1):
            v = v + ra[o].astype(F32)
        fa[...] = v.astype(BF16)
        rza[z] = v.astype(BF16)
        for o in range(1, nz):
            remote(fa, rza.at[z], at["a2"], along("z", nz, z, o)).start()

    def xy_third(stretch, own, me, got, out, last, size):
        lo, hi = stretches[stretch]
        def step(k, carry):
            zz = far(k)
            v = own[me, k].astype(F32)
            for o in range(size - 1):
                v = v + got[o, k].astype(F32)
            out[k] = v.astype(BF16)

            @pl.when(k < nz - 1)
            def _():
                o = lax.rem(zz - z + nz, nz)
                remote(out.at[k], last.at[o - 1], at["last"], {"z": zz}).start()

            return carry

        lax.fori_loop(lo, hi, step, 0)

    def third_both(stretch):
        lo, hi = stretches[stretch]
        part = rxy2.at[:, :, pl.ds(0, hi - lo)]
        remote(part, part, at["second"] + stretch, other).wait_recv()
        xy_third(stretch, sx, y, rx2, tx, rx3, ny)
        xy_third(stretch, sy, x, ry2, ty, ry3, nx)

    def z_third():
        remote(rz2, rz2, at["z2"], other).wait_recv()
        v = sz[x].astype(F32)
        for o in range(nx - 1):
            v = v + rz2[o].astype(F32)
        tz[...] = v.astype(BF16)
        for o in range(1, ny):
            peer = along("y", ny, y, o)
            remote(tz.at[peer["y"]], rz3.at[o - 1], at["z3"], peer).start()

    def small_line():
        rest = rza.at[pl.ds(0, nz - 1)]
        remote(rest, rest, at["a2"], other).wait_recv()
        v = rza[0].astype(F32)
        for zz in range(1, nz):
            v = v + rza[zz].astype(F32)
        fin[...] = v.astype(BF16)
        ag_a[place] = v.astype(BF16)
        for o in range(1, plane):
            remote(fin, ag_a.at[place], at["a3"], in_plane(o)).start()

    z_step(3, False)
    gather_both(0)

    @pl.when(line < count - 1)
    def _():
        height_copy.wait_recv()

    for b in range(blocks):
        tail = hh_r[:, lanes(b)].astype(F32)
        hg_v[b, rows:rows + HALO, :] = jnp.where(line == count - 1, 0.0, tail)

    loads["taps"].wait()

    def gated_block(b):
        lines = taps_v[:, lanes(b)].astype(F32)
        spread = [jnp.broadcast_to(lines[j:j + 1, :], (8, LANE)) for j in range(taps)]

        def step(t, carry):
            base = t * (8 * GROUP)
            acc = [None] * GROUP
            for k in range(taps + 8 * (GROUP - 1)):
                v = hg_v[b, pl.ds(base + k, 8), :]
                for u in range(GROUP):
                    j = reach + 8 * u - k
                    if 0 <= j < taps:
                        term = spread[j] * v
                        acc[u] = term if acc[u] is None else acc[u] + term
            for u in range(0, GROUP, 2):
                r = pl.ds(pl.multiple_of(base + 8 * u, 16), 16)
                g = jnp.concatenate(acc[u:u + 2], axis=0)
                s = sg_v[r, lanes(b)]
                gs = g * s
                gv_v[r, lanes(b)] = gs.astype(BF16)
                gg_v[r, lanes(b)] = (gs * cv_v[r, lanes(b)].astype(F32) * (1.0 - s)).astype(BF16)
            return carry

        lax.fori_loop(0, rows // (8 * GROUP), step, 0)

    for b in range(blocks):
        gated_block(b)
        if b == 1:
            z_step(3, True)
            gather_both(1)
        if b == 2:
            small_plane()
        if b == 3:
            z_done()
            third_both(0)
        if b == 4:
            third_both(1)
        if b == 5:
            small_line()
            z_third()

    remote(rxy3, rxy3, at["last"], other).wait_recv()
    for buf, own, last in ((0, tx, rx3), (1, ty, ry3)):
        v = own[nz - 1].astype(F32)
        for o in range(nz - 1):
            v = v + last[o].astype(F32)
        proj_v[:, buf * third:(buf + 1) * third] = v
    remote(rz3, rz3, at["z3"], other).wait_recv()
    v = tz[y].astype(F32)
    for o in range(ny - 1):
        v = v + rz3[o].astype(F32)
    proj_v[:, 2 * third:] = v

    rest = ag_a.at[pl.ds(0, plane - 1)]
    remote(rest, rest, at["a3"], other).wait_recv()
    for p in range(plane):
        stage[p * per:(p + 1) * per, :] = ag_a[p].astype(F32)
    for b in range(blocks):
        for j in range(taps + 2):
            row = b * (taps + 2) + j
            v = stage[row:row + 1, :]
            if j < taps:
                taps_o[j:j + 1, lanes(b)] = v
            else:
                (gain_o if j == taps else shift_o)[lanes(b)] = v.reshape(LANE)

    stat_copy.wait_send()

    @pl.when(line < count - 1)
    def _():
        gated_copy.wait_send()

    sums_copy.wait_send()

    @pl.when(line > 0)
    def _():
        height_copy.wait_send()

    for stretch, (lo, hi) in enumerate(stretches):
        some = pl.ds(0, hi - lo)
        for name, buf in (("far", fxy), ("near", rxy), ("second", rxy2)):
            part = buf.at[:, :, some]
            remote(part, part, at[name] + stretch, other).wait_send()
    for step in range(nz // 2):
        ring_wait(step, True).wait_send()
        if step > 0:
            ring_wait(step, False).wait_send()
    for name, part in (("last", rxy3), ("z2", rz2), ("z3", rz3), ("a1", ra), ("a2", rza.at[pl.ds(0, nz - 1)]), ("a3", rest)):
        remote(part, part, at[name], other).wait_send()


def local(conv_value, conv_gate, conv_out, conv_taps, norm_gain, norm_shift, proj_weight, out_grad):
    nz, ny, nx = (lax.axis_size(a) for a in SP)
    rows, chan = conv_value.shape
    depth = out_grad.shape[1]
    taps = conv_taps.shape[0]
    blocks = chan // LANE
    third = chan // 3
    plane = ny * nx
    slots, _ = layout(nz, ny, nx)
    vm = pltpu.VMEM
    per = -(-(blocks * (taps + 2)) // (16 * plane)) * 16
    scratch = [
        vm((rows, chan), BF16), vm((rows, depth), BF16), vm((depth, rows), BF16), vm((depth, chan), BF16), vm((rows, chan), BF16),
        vm((rows, chan), BF16), vm((taps, chan), BF16), vm((chan,), F32), vm((chan,), F32),
        vm((2, rows, LANE), F32), vm((2, rows, LANE), F32), vm((2, rows, LANE), F32), vm((2, rows, LANE), F32),
        vm((rows, LANE), F32), vm((rows, chan), F32), vm((blocks, rows + HALO, LANE), F32), vm((rows, chan), F32),
        vm((rows, chan), F32), vm((rows, chan), BF16), vm((rows, chan), F32), vm((blocks, rows + HALO, LANE), F32),
        vm((HALO, chan), BF16), vm((HALO, chan), BF16), vm((HALO, chan), BF16), vm((HALO, chan), BF16),
        vm((2, 4, nz, 4, 16, third), BF16), vm((nz, 4, 4, 16, third), BF16),
        vm((2, 2, nz, 2, 16, third), BF16), vm((2, 2, nz, 4, 16, third), BF16),
        vm((nz // 2, 4, 4, 16, third), BF16), vm((nz // 2, 4, 4, 16, third), BF16),
        vm((2, 4, nz, 16, third), BF16), vm((2, 3, nz, 16, third), BF16),
        vm((2, nz, 16, third), BF16), vm((2, nz - 1, 16, third), BF16),
        vm((nx, ny, 16, third), BF16), vm((nx - 1, ny, 16, third), BF16),
        vm((ny, 16, third), BF16), vm((ny - 1, 16, third), BF16),
        vm((plane * per, LANE), F32), vm((plane, per, LANE), BF16), vm((plane - 1, per, LANE), BF16), vm((per, LANE), BF16),
        vm((nz, per, LANE), BF16), vm((per, LANE), BF16), vm((plane, per, LANE), BF16),
        pltpu.SemaphoreType.DMA((8,)),
        pltpu.SemaphoreType.DMA((slots.used,)), pltpu.SemaphoreType.DMA((slots.used,)),
    ]
    anywhere = pl.BlockSpec(memory_space=pl.ANY)
    shapes = (
        ((rows, chan), BF16), ((rows, chan), BF16), ((taps, chan), F32), ((chan,), F32), ((chan,), F32), ((16, chan), F32),
    )
    held = pl.BlockSpec(memory_space=pltpu.VMEM)
    results = pl.pallas_call(
        functools.partial(kernel, (nz, ny, nx, rows, chan, depth, taps)),
        out_shape=tuple(pltpu.VMEM(*s) for s in shapes),
        in_specs=[anywhere] * 8,
        out_specs=(held,) * 6,
        scratch_shapes=scratch,
        compiler_params=pltpu.CompilerParams(
            collective_id=0, has_side_effects=True, vmem_limit_bytes=36 * 1024 * 1024),
        name="module_backward",
    )(*(pltpu.with_memory_space_constraint(a, pltpu.HBM) for a in (
        conv_value, conv_gate, conv_out, conv_taps, norm_gain, norm_shift, proj_weight, out_grad)))
    return pl.pallas_call(
        write_out,
        out_shape=tuple(jax.ShapeDtypeStruct(*s) for s in shapes),
        in_specs=[held] * 6,
        out_specs=(anywhere,) * 6,
        scratch_shapes=[pltpu.SemaphoreType.DMA((6,))],
        name="write_out",
    )(*(pltpu.with_memory_space_constraint(a, pltpu.VMEM) for a in results))


def write_out(*refs):
    sem = refs[12]
    copies = [pltpu.make_async_copy(refs[i], refs[6 + i], sem.at[i]) for i in range(6)]
    for c in copies:
        c.start()
    for c in copies:
        c.wait()


def solution(mesh):
    split = Mesh(mesh.devices.reshape(8, 4, 4, mesh.shape["tp"]), (*SP, "tp"))
    placed = (
        P(SP, "tp"), P(SP, "tp"), P(SP, "tp"), P(None, "tp"), P("tp"), P("tp"), P(None, "tp"), P(SP, None),
    )
    return jax.shard_map(
        local,
        mesh=split,
        in_specs=placed,
        out_specs=(P(SP, "tp"), P(SP, "tp"), P(None, "tp"), P("tp"), P("tp"), P(SP, "tp")),
        check_vma=False,
    )
```
